32 devices in a mesh: grp: 2 (over y), fs: 4 (over z), tp: 4 (over x, core).
Axes of the slice: x: 2, y: 2, z: 4, core: 2. Of those that a mesh axis runs over, the one named last changes fastest.
Arguments:
- tokens: bfloat16 [1024, 2048], P(('grp', 'fs'), 'tp'), parts along dimension 0, may hold values from -340 to 340
- routes: int32 [1024, 2], P(('grp', 'fs')), parts along dimension 0, may hold values from 0 to 7, all different within a row; in each aligned block of 128 rows (0 to 127, 128 to 255, ...) at most 40 rows name the same one
- route_weights: float32 [1024, 2], P(('grp', 'fs')), parts along dimension 0, may hold values from 0.2 to 1
- norm_gain: float32 [2048], P('fs'), may hold values from 0.1 to 1.9
- gate_weight: float32 [8, 2048, 4096], P(None, 'fs', 'tp'), may hold values from -0.125 to 0.125
- up_weight: float32 [8, 2048, 4096], P(None, 'fs', 'tp'), may hold values from -0.125 to 0.125
- down_weight: float32 [8, 2048, 4096], P(None, 'fs', 'tp'), may hold values from -0.09375 to 0.09375
Outputs:
- gate_out: bfloat16 [8, 4096, 4096], P('fs', 'grp', 'tp'), parts along dimension 1
- up_out: bfloat16 [8, 4096, 4096], P('fs', 'grp', 'tp'), parts along dimension 1
- down_out: bfloat16 [8, 4096, 4096], P('fs', 'grp', 'tp'), parts along dimension 1
- mixed_out: bfloat16 [1024, 2048], P(('grp', 'fs'), 'tp'), parts along dimension 0
The draws below stay inside these ranges and needn't reach their ends.
There are 2 independent parts, one for each index of `grp`. The reference program is written for one: setup_inputs(seed, part) draws one part's arguments, and reference() takes and returns one part's arrays. A program takes and returns all parts, laid end to end along the dimension named above; an argument that names none is the same for every part. Nothing has to cross between parts.
Inputs may be any that keep to these rules, and one draw needn't show every extreme that they name: `routes`: each row names 2 different experts; in each aligned block of 128 rows no expert is named by more than 40 rows, and in some block one expert is named by exactly 40 rows.
All inputs are finite; a program needn't handle non-finite values.
Results may differ from the reference program's by a relative error of at most 0.015.
Values may be sent and summed in bfloat16 or wider, within the bound.
A program may use at most 192 MiB of HBM per device.

```python
import math
import jax
import jax.numpy as jnp
import numpy as np
from jax import lax

D = 2048
FF = 4096
EXPERTS = 8
TOP = 2
TOK_FS = 128
CAP = 40
SUB = 1
FFS = 1024
TOKENS = 512
N_FS = 4
N_TP = 4


def draw_tokens(key, part):
    noise_key, column_key, row_key = jax.random.split(key, 3)
    columns = jnp.arange(D, dtype=jnp.float32) / D
    column_scale = jnp.exp(math.log(4.0) * columns) * jax.random.uniform(column_key, (D,), jnp.float32, 0.6, 1.4)
    row_scale = jnp.exp(jax.random.uniform(row_key, (TOKENS, 1), jnp.float32, 0.0, math.log(10.0)))
    values = jnp.clip(jax.random.normal(noise_key, (TOKENS, D), jnp.float32), -6.0, 6.0)
    return (values * column_scale[None, :] * row_scale).astype(jnp.bfloat16)


def block_levels(stream_key, extent, cuts, least, top_value):
    loudness, own = 1.0, jax.random.fold_in(stream_key, 6)
    for axis_at, shards_of in cuts:
        steps = jnp.exp(jax.random.uniform(jax.random.fold_in(own, axis_at), (shards_of,), jnp.float32, least / len(cuts), top_value / len(cuts)))
        loudness = loudness * jnp.repeat(steps, extent[axis_at] // shards_of).reshape([-1 if axis == axis_at else 1 for axis in range(len(extent))])
    return loudness


def assign_block(own_key, own, number, rows, count, top, limit, skew):
    order = jax.random.permutation(own_key, count)
    crowded, ordinary = shares(count, rows * top, limit, skew, True), shares(count, rows * top, limit, skew, False)
    places = jnp.arange(count)

    def named(sizes, rotation):
        used = int((sizes > 0).sum())
        fixed = max(1, used // 4)
        shifted = fixed + (places - fixed + rotation * (used - fixed)) % max(1, count - fixed)
        return jnp.zeros((count,), jnp.int32).at[order[jnp.where(places < fixed, places, shifted)]].set(jnp.asarray(sizes, jnp.int32))

    sizes = jnp.where(number % 4 == 0, named(crowded, number // 4), named(ordinary, number - number // 4 - 1))
    mixed = jax.random.permutation(jax.random.fold_in(own, 3), count)
    donor, taker = mixed[0:count // 2 * 2:2], mixed[1:count // 2 * 2:2]
    slack = jnp.minimum(sizes[donor] - 1, limit - sizes[taker]) // 2
    slack = jnp.where((donor == order[0]) | (taker == order[0]) | (sizes[taker] == 0), 0, jnp.maximum(slack, 0))
    shifted = jax.random.randint(jax.random.fold_in(own, 4), (count // 2,), 0, 1 << 20) % (slack + 1)
    sizes = sizes.at[donor].add(-shifted).at[taker].add(shifted)
    members = jnp.searchsorted(jnp.cumsum(sizes), jnp.arange(rows * top), side="right").astype(jnp.int32)
    table = members.reshape(top, rows).T
    table = table[jax.random.permutation(jax.random.fold_in(own, 1), rows)]
    rotation = jax.random.randint(jax.random.fold_in(own, 2), (rows, 1), 0, top)
    return jnp.take_along_axis(table, (jnp.arange(top)[None, :] + rotation) % top, axis=1)


def shares(count, total, reach, skew, full):
    portions = [(1 << 20) // math.isqrt(rank ** skew) + 1 for rank in range(1, count + 1)]
    largest = reach if full else min(reach, max(-(-total // count), total * portions[0] // sum(portions)))
    least = 1 if total - largest >= count - 1 else 0
    holding, spare = [largest] + [least] * (count - 1), total - largest - least * (count - 1)
    while spare > 0:
        free = [i for i in range(1, count) if holding[i] < largest] or [i for i in range(1, count) if holding[i] < reach]
        mass, budget = sum([portions[i] for i in free]), spare
        for i in free:
            addition = min(reach - holding[i], max(1, budget * portions[i] // mass), spare)
            holding[i] = holding[i] + addition
            spare = spare - addition
    return np.array(holding)


def scatter_about(own_key, dims, scale, reach, cuts=(), kind=jnp.bfloat16):
    result = scale * jax.random.normal(own_key, dims, jnp.float32)
    if cuts:
        result = result * block_levels(own_key, dims, cuts, -0.22, 0.18)
    return jnp.clip(result, -reach, reach).astype(kind)


def setup_inputs(seed: int = 0, part: int = 0) -> dict:
    seeds = jax.random.split(jax.random.key(seed), 8)
    own_keys = jax.random.split(jax.random.fold_in(seeds[7], part), 8)
    tokens = draw_tokens(jax.random.fold_in(jax.random.fold_in(seeds[7], part), 71), part)
    routes_keys = jax.random.split(jax.random.fold_in(own_keys[1], 1), TOKENS // TOK_FS)
    routes_turns = jax.random.permutation(jax.random.fold_in(own_keys[1], 3), TOKENS // TOK_FS)
    routes = jax.vmap(lambda own, number: assign_block(jax.random.fold_in(own_keys[1], 2), own, number, TOK_FS, EXPERTS, TOP, CAP, 1))(routes_keys, routes_turns).reshape((TOKENS, TOP))
    route_weights = jnp.clip(0.2 + 0.8 * jax.random.uniform(own_keys[2], (TOKENS, TOP), jnp.float32) ** block_levels(own_keys[2], (TOKENS, TOP), ((0, 4),), -0.2, 0.2), 0.2, 1.0)
    norm_gain = jnp.clip(1.0 + 0.18 * jax.random.normal(seeds[3], (D,), jnp.float32), 0.1, 1.9)
    gate_weight = scatter_about(seeds[4], (EXPERTS, D, FF), D ** -0.5, 0.125, ((1, 4), (2, 4)), jnp.float32)
    up_weight = scatter_about(seeds[5], (EXPERTS, D, FF), D ** -0.5, 0.125, ((1, 4), (2, 4)), jnp.float32)
    down_weight = scatter_about(seeds[6], (EXPERTS, D, FF), FF ** -0.5, 0.09375, ((1, 4), (2, 4)), jnp.float32)
    return {"tokens": tokens, "routes": routes, "route_weights": route_weights, "norm_gain": norm_gain, "gate_weight": gate_weight, "up_weight": up_weight, "down_weight": down_weight}


epsilon = 1e-06

def relayout(matrix):
    blocked = matrix.reshape(EXPERTS, D, N_TP, SUB, FFS)
    return jnp.transpose(blocked, (0, 3, 1, 2, 4)).reshape(EXPERTS * SUB, D, N_TP * FFS)

def slot_table(routes):
    blocks = routes.reshape(N_FS, TOK_FS * TOP)
    onehot = (blocks[:, :, None] == jnp.arange(EXPERTS, dtype=jnp.int32)[None, None, :]).astype(jnp.int32)
    earlier = jnp.cumsum(onehot, axis=1) - onehot
    position = lax.optimization_barrier(jnp.sum(earlier * onehot, axis=2))
    block_index = jnp.arange(N_FS, dtype=jnp.int32)[:, None]
    return (block_index * CAP + position).astype(jnp.int32).reshape(TOKENS, TOP)

def reference(tokens, routes, route_weights, norm_gain, gate_weight, up_weight, down_weight):
    gain_row = norm_gain[None, :, None]
    gate_fold = (gain_row * gate_weight).astype(jnp.bfloat16)
    up_fold = (gain_row * up_weight).astype(jnp.bfloat16)
    down_cast = down_weight.astype(jnp.bfloat16)
    widened = tokens.astype(jnp.float32)
    row_scale = lax.rsqrt(lax.optimization_barrier(jnp.mean(widened * widened, axis=1, keepdims=True)) + epsilon)
    normed = (widened * row_scale).astype(jnp.bfloat16)
    slot_place = slot_table(routes)
    token_ids = jnp.broadcast_to(jnp.arange(TOKENS, dtype=jnp.int32)[:, None], (TOKENS, TOP))
    owner_rows = jnp.zeros((EXPERTS, N_FS * CAP), jnp.int32).at[routes, slot_place].set(token_ids)

    def one_expert(expert_args):
        gate_expert, up_expert, down_expert, owner_expert = expert_args
        token_rows = normed[owner_expert]
        gate_sums = jnp.dot(token_rows, gate_expert, preferred_element_type=jnp.float32)
        up_sums = jnp.dot(token_rows, up_expert, preferred_element_type=jnp.float32)
        hidden = (jax.nn.silu(gate_sums) * up_sums).astype(jnp.bfloat16)
        blocks = hidden.reshape(N_FS * CAP, SUB * N_TP, FFS).astype(jnp.float32)
        down_blocks = down_expert.reshape(D, SUB * N_TP, FFS).astype(jnp.float32)
        partial_value = jnp.einsum('mbf,dbf->bmd', blocks, down_blocks).astype(jnp.bfloat16)
        return lax.optimization_barrier(jnp.sum(partial_value.astype(jnp.float32), axis=0))
    results = lax.map(one_expert, (gate_fold, up_fold, down_cast, owner_rows))
    selected = results[routes, slot_place]
    mixed_rows = lax.optimization_barrier(jnp.sum(route_weights[:, :, None] * selected, axis=1)).astype(jnp.bfloat16)
    return (relayout(gate_fold), relayout(up_fold), relayout(down_cast), mixed_rows)
```

```python
import functools

import jax
import jax.numpy as jnp
from jax import lax
from jax.experimental import pallas as pl
from jax.experimental.pallas import tpu as pltpu
from jax.sharding import PartitionSpec as P

epsilon = 1e-06
MESH = pl.DeviceIdType.MESH


def expert_slots(routes, experts, capacity):
    row_count = routes.shape[0] * routes.shape[1]
    flat_routes = routes.reshape(row_count)
    onehot = (flat_routes[:, None] == jnp.arange(experts, dtype=jnp.int32)[None, :]).astype(
        jnp.int32
    )
    earlier = jnp.cumsum(onehot, axis=0) - onehot
    position = jnp.sum(earlier * onehot, axis=1)
    return (flat_routes * capacity + position).reshape(routes.shape)


def dispatch(normed, slots, experts, capacity, copies, local_count):
    col_width = normed.shape[1]
    slot_ids = jnp.arange(experts * capacity, dtype=jnp.int32)
    select = jnp.any(slot_ids[:, None, None] == slots[None, :, :], axis=2).astype(jnp.bfloat16)
    packed = jnp.dot(select, normed, preferred_element_type=jnp.float32).astype(jnp.bfloat16)
    packed = jnp.broadcast_to(
        packed.reshape(experts, 1, capacity, col_width), (experts, copies, capacity, col_width)
    )
    return packed.reshape(experts * copies // local_count, local_count, capacity, col_width)


def combine(returned, slots, route_weights, experts, copies):
    capacity, col_width = (returned.shape[2], returned.shape[3])
    summed_up = jnp.sum(
        returned.reshape(experts, copies, capacity, col_width), axis=1, dtype=jnp.float32
    )
    selected = summed_up.reshape(experts * capacity, col_width)[slots]
    return jnp.sum(route_weights[:, :, None] * selected, axis=1)


def exchange_kernel(
    dims, gains, gate_w, up_w, down_w, gate_o, up_o, down_o,
    raw, stage, load_sem, send_sem, recv_sem, pass_send, pass_recv,
):
    groups, count, local, copies, rows, width, parts = dims
    weights, landing = (gate_w, up_w, down_w), (gate_o, up_o, down_o)
    y, z = lax.axis_index("grp"), lax.axis_index("fs")
    share = rows // groups
    piece = share // parts

    barrier = pltpu.get_barrier_semaphore()

    def greet(j, _):
        @pl.when(j != z)
        def _():
            pl.semaphore_signal(barrier, inc=1, device_id={"fs": j}, device_id_type=MESH)
        return 0

    lax.fori_loop(0, count, greet, 0)
    for other in range(1, groups):
        pl.semaphore_signal(
            barrier, inc=1, device_id={"grp": lax.rem(y + other, groups)}, device_id_type=MESH
        )

    def load(m, j, first, slot):
        if copies > 1:
            expert, column = j // copies, lax.rem(j, copies) * width
            column = pl.ds(pl.multiple_of(column, 128), width)
        else:
            expert, column = j * local, slice(None)
        return pltpu.make_async_copy(
            weights[m].at[pl.ds(expert, local), pl.ds(first, share), column],
            raw.at[slot], load_sem.at[slot],
        )

    def fold(m, slot, first, put):
        def one(i, _):
            l, q = i // parts, lax.rem(i, parts)
            at = pl.multiple_of(q * piece, piece)
            scaled = raw[slot, l, pl.ds(at, piece), :]
            if m < 2:
                scaled = scaled * gains[pl.ds(pl.multiple_of(first + at, piece), piece), :1]
            put(l, at, scaled.astype(jnp.bfloat16))
            return 0

        lax.fori_loop(0, local * parts, one, 0)

    def sending(j, m, i):
        l, q = i // parts, lax.rem(i, parts)
        at = pl.multiple_of(q * piece, piece)
        base = pl.multiple_of(z * rows + y * share + at, piece)
        return pltpu.make_async_remote_copy(
            src_ref=stage.at[j, m, l, pl.ds(at, piece), :],
            dst_ref=landing[m].at[l, pl.ds(base, piece), :],
            send_sem=send_sem.at[j, m, i],
            recv_sem=recv_sem.at[z, m, i],
            device_id={"fs": j}, device_id_type=MESH,
        )

    def passing(s, m, i, other):
        l, q = i // parts, lax.rem(i, parts)
        base = pl.multiple_of(s * rows + y * share + q * piece, piece)
        spot = landing[m].at[l, pl.ds(base, piece), :]
        return pltpu.make_async_remote_copy(
            src_ref=spot, dst_ref=spot,
            send_sem=pass_send.at[s, m, i, other - 1],
            recv_sem=pass_recv.at[s, m, i, other - 1],
            device_id={"grp": lax.rem(y + other, groups)}, device_id_type=MESH,
        )

    def arriving(s, m, i, other):
        l, q = i // parts, lax.rem(i, parts)
        giver = lax.rem(y + groups - other, groups)
        base = pl.multiple_of(s * rows + giver * share + q * piece, piece)
        spot = landing[m].at[l, pl.ds(base, piece), :]
        return pltpu.make_async_remote_copy(
            src_ref=spot, dst_ref=spot,
            send_sem=pass_send.at[s, m, i, other - 1],
            recv_sem=pass_recv.at[s, m, i, other - 1],
            device_id={"grp": giver}, device_id_type=MESH,
        )

    def landed(s, m, i):
        l, q = i // parts, lax.rem(i, parts)
        base = pl.multiple_of(s * rows + y * share + q * piece, piece)
        return pltpu.make_async_remote_copy(
            src_ref=landing[m].at[l, pl.ds(base, piece), :],
            dst_ref=landing[m].at[l, pl.ds(base, piece), :],
            send_sem=send_sem.at[s, m, i],
            recv_sem=recv_sem.at[s, m, i],
            device_id={"fs": s}, device_id_type=MESH,
        )

    mine = pl.multiple_of(y * share, share)
    pieces = local * parts

    def neighbours(body):
        def step(d, _):
            for j, there in ((z + d, z + d < count), (z - d, z - d >= 0)):
                @pl.when(there)
                def _():
                    body(j)
            return 0

        lax.fori_loop(1, count, step, 0)

    def send_phase(phase):
        def to(j):
            for m in phase:
                load(m, j, mine, m % 2).start()
            for m in phase:
                load(m, j, mine, m % 2).wait()

                def put(l, at, value):
                    stage[j, m, l, pl.ds(at, piece), :] = value

                fold(m, m % 2, mine, put)
            for m in phase:
                def go(i, _):
                    sending(j, m, i).start()
                    return 0

                lax.fori_loop(0, pieces, go, 0)

        neighbours(to)

    pl.semaphore_wait(barrier, count - 1 + groups - 1)
    send_phase((0, 1))
    send_phase((2,))

    for m in range(3):
        for g in range(groups):
            load(m, z, g * share, g % 2).start()
            load(m, z, g * share, g % 2).wait()

            def put(l, at, value):
                base = pl.multiple_of(z * rows + g * share + at, piece)
                landing[m][l, pl.ds(base, piece), :] = value

            fold(m, g % 2, g * share, put)

    def pass_phase(phase):
        def take(s):
            for m in phase:
                def one(i, _):
                    landed(s, m, i).wait_recv()
                    for other in range(1, groups):
                        passing(s, m, i, other).start()
                    return 0

                lax.fori_loop(0, pieces, one, 0)

        neighbours(take)

    pass_phase((0, 1))
    pass_phase((2,))

    def finish(s):
        for m in range(3):
            def one(i, _):
                for other in range(1, groups):
                    arriving(s, m, i, other).wait_recv()
                    passing(s, m, i, other).wait_send()
                sending(s, m, i).wait_send()
                return 0

            lax.fori_loop(0, pieces, one, 0)

    neighbours(finish)


def relay_kernel(
    dims, gains, gate_w, up_w, down_w, gate_o, up_o, down_o,
    raw, stage, transit, load_sem, send_sem, recv_sem, relay_sem, pass_send, pass_recv,
):
    groups, count, local, copies, rows, width, parts = dims
    weights, landing = (gate_w, up_w, down_w), (gate_o, up_o, down_o)
    y, z = lax.axis_index("grp"), lax.axis_index("fs")
    share = rows // groups
    piece = share // parts
    pieces = local * parts
    mine = pl.multiple_of(y * share, share)

    def real(way, place):
        return place if way == 0 else count - 1 - place

    barrier = pltpu.get_barrier_semaphore()
    for j, there in ((z + 1, z + 1 < count), (z - 1, z >= 1)):
        @pl.when(there)
        def _():
            pl.semaphore_signal(barrier, inc=1, device_id={"fs": j}, device_id_type=MESH)
    for other in range(1, groups):
        pl.semaphore_signal(
            barrier, inc=1, device_id={"grp": lax.rem(y + other, groups)}, device_id_type=MESH
        )

    def load(m, j, first, slot):
        if copies > 1:
            expert, column = j // copies, lax.rem(j, copies) * width
            column = pl.ds(pl.multiple_of(column, 128), width)
        else:
            expert, column = j * local, slice(None)
        return pltpu.make_async_copy(
            weights[m].at[pl.ds(expert, local), pl.ds(first, share), column],
            raw.at[slot], load_sem.at[slot],
        )

    def cut(i):
        return i // parts, pl.multiple_of(lax.rem(i, parts) * piece, piece)

    def fold(m, slot, first, put):
        def one(i, _):
            l, at = cut(i)
            scaled = raw[slot, l, pl.ds(at, piece), :]
            if m < 2:
                scaled = scaled * gains[pl.ds(pl.multiple_of(first + at, piece), piece), :1]
            put(l, at, scaled.astype(jnp.bfloat16))
            return 0

        lax.fori_loop(0, pieces, one, 0)

    def spot(m, l, at, source, giver):
        base = pl.multiple_of(source * rows + giver * share + at, piece)
        return landing[m].at[l, pl.ds(base, piece), :]

    def hop(way, src, sem, m, i, k, s, dd, final):
        l, at = cut(i)
        if final:
            dst = spot(m, l, at, real(way, s), y)
        else:
            slot = (k - s) * (count - 2 - k) + (count - 1 - dd)
            dst = transit.at[way, slot, m, l, pl.ds(at, piece), :]
        place = (k - s) * (count - 1 - k) + (count - 1 - dd)
        return pltpu.make_async_remote_copy(
            src_ref=src, dst_ref=dst, send_sem=sem,
            recv_sem=recv_sem.at[way, place, m, i],
            device_id={"fs": real(way, k + 1)}, device_id_type=MESH,
        )

    def start_hop(way, src, sem, m, i, k, s, dd):
        @pl.when(dd == k + 1)
        def _():
            hop(way, src, sem, m, i, k, s, dd, True).start()

        @pl.when(dd > k + 1)
        def _():
            hop(way, src, sem, m, i, k, s, dd, False).start()

    def passing(s, m, i, other):
        l, at = cut(i)
        ref = spot(m, l, at, s, y)
        return pltpu.make_async_remote_copy(
            src_ref=ref, dst_ref=ref,
            send_sem=pass_send.at[s, m, i, other - 1],
            recv_sem=pass_recv.at[s, m, i, other - 1],
            device_id={"grp": lax.rem(y + other, groups)}, device_id_type=MESH,
        )

    def arriving(s, m, i, other):
        l, at = cut(i)
        giver = lax.rem(y + groups - other, groups)
        ref = spot(m, l, at, s, giver)
        return pltpu.make_async_remote_copy(
            src_ref=ref, dst_ref=ref,
            send_sem=pass_send.at[s, m, i, other - 1],
            recv_sem=pass_recv.at[s, m, i, other - 1],
            device_id={"grp": giver}, device_id_type=MESH,
        )

    def send_phase(phase):
        def step(d, _):
            for way in (0, 1):
                k = real(way, z)
                dd = count - d
                j = real(way, dd)

                @pl.when(dd > k)
                def _():
                    for m in phase:
                        load(m, j, mine, m).start()
                    for m in phase:
                        load(m, j, mine, m).wait()

                        def put(l, at, value):
                            stage[j, m, l, pl.ds(at, piece), :] = value

                        fold(m, m, mine, put)

                        def go(i, _):
                            l, at = cut(i)
                            src = stage.at[j, m, l, pl.ds(at, piece), :]
                            start_hop(way, src, send_sem.at[j, m, i], m, i, k, k, dd)
                            return 0

                        lax.fori_loop(0, pieces, go, 0)
            return 0

        lax.fori_loop(1, count, step, 0)

    def own_block():
        for m in range(3):
            for g in range(groups):
                load(m, z, g * share, g % 2).start()
                load(m, z, g * share, g % 2).wait()

                def put(l, at, value):
                    stage[z, m, l, pl.ds(at, piece), :] = value

                fold(m, g % 2, g * share, put)
                base = pl.multiple_of(z * rows + g * share, share)
                keep = pltpu.make_async_copy(
                    stage.at[z, m], landing[m].at[:, pl.ds(base, share), :], load_sem.at[g % 2]
                )
                keep.start()
                keep.wait()

    def take_phase(phase):
        most = max(k * (count - k) for k in range(count))

        def take(item, _):
            for m in phase:
                def one(i, _):
                    l, at = cut(i)
                    for way in (0, 1):
                        take_piece(way, m, item, i, l, at)
                    return 0

                lax.fori_loop(0, pieces, one, 0)
            return 0

        lax.fori_loop(0, most, take, 0)

    def take_piece(way, m, item, i, l, at):
        k = real(way, z)

        @pl.when(item < k * (count - k))
        def _():
            s = k - 1 - item // (count - k)
            dd = count - 1 - lax.rem(item, count - k)
            source = real(way, s)

            def awaited(ref):
                pltpu.make_async_remote_copy(
                    src_ref=ref, dst_ref=ref, send_sem=send_sem.at[source, m, i],
                    recv_sem=recv_sem.at[way, item, m, i],
                    device_id={"fs": source}, device_id_type=MESH,
                ).wait_recv()

            @pl.when(dd == k)
            def _():
                awaited(spot(m, l, at, source, y))
                for other in range(1, groups):
                    passing(source, m, i, other).start()

            @pl.when(dd > k)
            def _():
                slot = (k - 1 - s) * (count - 1 - k) + (count - 1 - dd)
                ref = transit.at[way, slot, m, l, pl.ds(at, piece), :]
                awaited(ref)
                start_hop(way, ref, relay_sem.at[way, slot, m, i], m, i, k, s, dd)

    def sent(ref, sem):
        pltpu.make_async_remote_copy(
            src_ref=ref, dst_ref=ref, send_sem=sem, recv_sem=recv_sem.at[0, 0, 0, 0],
            device_id={"grp": lax.rem(y + 1, groups)}, device_id_type=MESH,
        ).wait_send()

    def finish():
        def block(t, _):
            s, i = t // pieces, lax.rem(t, pieces)
            l, at = cut(i)

            @pl.when(s != z)
            def _():
                for m in range(3):
                    for other in range(1, groups):
                        arriving(s, m, i, other).wait_recv()
                        passing(s, m, i, other).wait_send()
                    sent(stage.at[s, m, l, pl.ds(at, piece), :], send_sem.at[s, m, i])
            return 0

        lax.fori_loop(0, count * pieces, block, 0)

        def passed(t, _):
            slot, i = t // pieces, lax.rem(t, pieces)
            l, at = cut(i)
            for way in (0, 1):
                @pl.when(slot < z * (count - 1 - z))
                def _():
                    for m in range(3):
                        sent(
                            transit.at[way, slot, m, l, pl.ds(at, piece), :],
                            relay_sem.at[way, slot, m, i],
                        )
            return 0

        lax.fori_loop(0, transit.shape[1] * pieces, passed, 0)

    ends = (z == 0).astype(jnp.int32) + (z == count - 1).astype(jnp.int32)
    pl.semaphore_wait(barrier, 2 - ends + groups - 1)
    send_phase((0, 1, 2))
    own_block()
    take_phase((0, 1, 2))
    finish()


def exchange(norm_gain, gate_weight, up_weight, down_weight, groups, count, copies, local):
    experts, rows, columns = gate_weight.shape
    width = columns // copies
    share = rows // groups
    parts = max(1, share // 128)
    gains = jnp.broadcast_to(norm_gain[:, None], (rows, 128))
    shape = (local, count * rows, width)
    dims = (groups, count, local, copies, rows, width, parts)
    pieces = local * parts
    relaying = 1 < count <= 8 and groups > 1
    common = [
        pltpu.VMEM((3, local, share, width), jnp.float32),
        pltpu.VMEM((count, 3, local, share, width), jnp.bfloat16),
    ]
    sem = pltpu.SemaphoreType.DMA
    passes = [sem((count, 3, pieces, max(1, groups - 1)))] * 2
    if relaying:
        slots = max(1, max(k * (count - 1 - k) for k in range(count)))
        items = max(k * (count - k) for k in range(count))
        scratch = common + [
            pltpu.VMEM((2, slots, 3, local, share, width), jnp.bfloat16),
            sem((3,)), sem((count, 3, pieces)), sem((2, items, 3, pieces)),
            sem((2, slots, 3, pieces)),
        ] + passes
    else:
        scratch = common + [sem((2,))] + [sem((count, 3, pieces))] * 2 + passes
    return pl.pallas_call(
        functools.partial(relay_kernel if relaying else exchange_kernel, dims),
        out_shape=[jax.ShapeDtypeStruct(shape, jnp.bfloat16)] * 3,
        in_specs=[pl.BlockSpec(memory_space=pltpu.VMEM)]
        + [pl.BlockSpec(memory_space=pl.ANY)] * 3,
        out_specs=[pl.BlockSpec(memory_space=pl.ANY if relaying else pltpu.VMEM)] * 3,
        scratch_shapes=scratch,
        compiler_params=pltpu.CompilerParams(
            collective_id=0, has_side_effects=True, vmem_limit_bytes=60 * 1024 * 1024
        ),
    )(gains, gate_weight, up_weight, down_weight)


def layered(tokens, routes, route_weights, norm_gain, gate_weight, up_weight, down_weight):
    groups = lax.axis_size("grp")
    fs_count = lax.axis_size("fs")
    tp_count = lax.axis_size("tp")
    experts = gate_weight.shape[0]
    copies = max(1, fs_count // experts)
    local_count = max(1, experts // fs_count)
    capacity = tokens.shape[0] * 5 // 16

    gate_new, up_new, down_new = exchange(
        norm_gain, gate_weight, up_weight, down_weight, groups, fs_count, copies, local_count
    )
    slots = expert_slots(routes, experts, capacity)
    whole = lax.all_gather(tokens, "tp", axis=1, tiled=True)
    widened = whole.astype(jnp.float32)
    row_scale = lax.rsqrt(jnp.mean(widened * widened, axis=1, keepdims=True) + epsilon)
    normed = (widened * row_scale).astype(jnp.bfloat16)
    outgoing = dispatch(normed, slots, experts, capacity, copies, local_count)
    arrived = lax.all_to_all(outgoing, "fs", split_axis=0, concat_axis=0, tiled=True)
    gate_sums = jnp.einsum("slcd,ldf->slcf", arrived, gate_new, preferred_element_type=jnp.float32)
    up_sums = jnp.einsum("slcd,ldf->slcf", arrived, up_new, preferred_element_type=jnp.float32)
    hidden = (jax.nn.silu(gate_sums) * up_sums).astype(jnp.bfloat16)
    partial_value = jnp.einsum(
        "slcf,ldf->slcd", hidden, down_new, preferred_element_type=jnp.float32
    ).astype(jnp.bfloat16)
    by_columns = partial_value.reshape(
        partial_value.shape[:3] + (tp_count, partial_value.shape[3] // tp_count)
    )
    exchanged = lax.all_to_all(by_columns, "tp", split_axis=3, concat_axis=3, tiled=True)
    summed_up = jnp.sum(exchanged, axis=3, dtype=jnp.float32)
    handed = lax.all_to_all(
        summed_up.astype(jnp.bfloat16), "fs", split_axis=0, concat_axis=0, tiled=True
    ).astype(summed_up.dtype)
    combined = combine(handed, slots, route_weights, experts, copies)
    return (gate_new, up_new, down_new, combined.astype(jnp.bfloat16))


def far_first(count):
    table = []
    for z in range(count):
        right = [j for j in range(count - 1, z, -1)]
        left = [j for j in range(z)]
        ways, order = sorted((right, left), key=len, reverse=True), []
        for d in range(count):
            order += [way[d] for way in ways if d < len(way)]
        table.append(order)
    return table


def fused_kernel(
    dims, tokens, routes, route_weights, gains, gate_w, up_w, down_w,
    gate_o, up_o, down_o, mixed_o, transit,
    raw, stage, gain_col, scales, send_x, land_x, normed, sums, hidden, partial, summing, combine_w,
    send_ret, land_ret,
    load_sem, send_sem, recv_sem, relay_sem, pass_send, pass_recv,
    x_send, x_recv, xg_send, xg_recv, part_send, part_recv, ret_send, ret_recv,
):
    groups, count, tps, local, rows, width, parts, experts, capacity = dims
    weights, landing = (gate_w, up_w, down_w), (gate_o, up_o, down_o)
    y, z, t = lax.axis_index("grp"), lax.axis_index("fs"), lax.axis_index("tp")
    share = rows // groups
    piece = share // parts
    pieces = local * parts
    mine = pl.multiple_of(y * share, share)
    table = far_first(count)
    block_rows = local * capacity
    own_tokens, columns = tokens.shape
    tall = count * capacity
    f32, bf16 = jnp.float32, jnp.bfloat16

    def ranked(r):
        return sum((z == k).astype(jnp.int32) * table[k][r] for k in range(count))

    def real(way, place):
        return place if way == 0 else count - 1 - place

    def remote(src, dst, send, recv, axis, index):
        return pltpu.make_async_remote_copy(
            src_ref=src, dst_ref=dst, send_sem=send, recv_sem=recv,
            device_id={axis: index}, device_id_type=MESH,
        )

    barrier = pltpu.get_barrier_semaphore()
    for axis, me, size in (("fs", z, count), ("grp", y, groups), ("tp", t, tps)):
        for other in range(1, size):
            pl.semaphore_signal(
                barrier, inc=1, device_id={axis: lax.rem(me + other, size)}, device_id_type=MESH
            )

    def load(m, j, first, slot):
        return pltpu.make_async_copy(
            weights[m].at[pl.ds(j * local, local), pl.ds(first, share), :],
            raw.at[slot], load_sem.at[slot],
        )

    def cut(i):
        return i // parts, pl.multiple_of(lax.rem(i, parts) * piece, piece)

    def fold(m, slot, first, put):
        def one(i, _):
            l, at = cut(i)
            scaled = raw[slot, l, pl.ds(at, piece), :]
            if m < 2:
                scaled = scaled * gain_col[pl.ds(pl.multiple_of(first + at, piece), piece), :1]
            put(l, at, scaled.astype(bf16))
            return 0

        lax.fori_loop(0, pieces, one, 0)

    def spot(m, l, at, source, giver):
        base = pl.multiple_of(source * rows + giver * share + at, piece)
        return landing[m].at[l, pl.ds(base, piece), :]

    def start_hop(way, src, sem, m, i, k, s, dd):
        l, at = cut(i)
        place = (k - s) * (count - 1 - k) + (count - 1 - dd)
        recv = recv_sem.at[way, place, m, i]

        @pl.when(dd == k + 1)
        def _():
            remote(src, spot(m, l, at, real(way, s), y), sem, recv, "fs", real(way, k + 1)).start()

        @pl.when(dd > k + 1)
        def _():
            slot = (k - s) * (count - 2 - k) + (count - 1 - dd)
            dst = transit.at[way, slot, m, l, pl.ds(at, piece), :]
            remote(src, dst, sem, recv, "fs", real(way, k + 1)).start()

    def passing(s, m, i, other):
        l, at = cut(i)
        ref = spot(m, l, at, s, y)
        return remote(
            ref, ref, pass_send.at[s, m, i, other - 1], pass_recv.at[s, m, i, other - 1],
            "grp", lax.rem(y + other, groups),
        )

    def arriving(s, m, i, other):
        l, at = cut(i)
        giver = lax.rem(y + groups - other, groups)
        ref = spot(m, l, at, s, giver)
        return remote(
            ref, ref, pass_send.at[s, m, i, other - 1], pass_recv.at[s, m, i, other - 1],
            "grp", giver,
        )

    def slot_rows():
        wanted = routes[...]
        expert_ids = lax.broadcasted_iota(jnp.int32, (experts, own_tokens), 0)
        onehots = [
            (expert_ids == wanted[k : k + 1, :]).astype(f32) for k in range(wanted.shape[0])
        ]
        before = lax.broadcasted_iota(jnp.int32, (own_tokens, own_tokens), 0)
        after = lax.broadcasted_iota(jnp.int32, (own_tokens, own_tokens), 1)
        upper = (before < after).astype(bf16)
        earlier = jnp.dot(sum(onehots).astype(bf16), upper, preferred_element_type=f32)
        found = []
        for k, onehot in enumerate(onehots):
            position = jnp.sum(earlier * onehot, axis=0, keepdims=True)
            earlier = earlier + onehot
            found.append(wanted[k : k + 1, :] * capacity + position.astype(jnp.int32))
        return found

    def pack():
        found = slot_rows()
        slot_ids = lax.broadcasted_iota(jnp.int32, (experts * capacity, own_tokens), 0)
        chosen = jnp.zeros((experts * capacity, own_tokens), f32)
        weighed = jnp.zeros((experts * capacity, own_tokens), f32)
        for k, slot in enumerate(found):
            hit = slot_ids == slot
            chosen = jnp.where(hit, 1.0, chosen)
            weighed = weighed + jnp.where(hit, route_weights[k : k + 1, :], 0.0)
        packed = jnp.dot(chosen.astype(bf16), tokens[...], preferred_element_type=f32)
        packed = packed.astype(bf16)
        for j in range(count):
            send_x[j] = packed[j * block_rows : (j + 1) * block_rows, :]
        high = weighed.astype(bf16)
        combine_w[0] = high
        combine_w[1] = (weighed - high.astype(f32)).astype(bf16)

    def dispatching(j):
        return remote(send_x.at[j], land_x.at[t, z], x_send.at[j], x_recv.at[z], "fs", j)

    def dispatched(s):
        return remote(send_x.at[s], land_x.at[t, s], x_send.at[s], x_recv.at[s], "fs", s)

    def spreading(s, other):
        return remote(
            land_x.at[t, s], land_x.at[t, s], xg_send.at[other, s], xg_recv.at[t, s],
            "tp", lax.rem(t + other, tps),
        )

    def spread(s, peer):
        return remote(
            land_x.at[peer, s], land_x.at[peer, s], xg_send.at[0, s], xg_recv.at[peer, s],
            "tp", peer,
        )

    def elsewhere(body):
        for other in range(1, count):
            body(lax.rem(z + other, count))

    def normalise():
        for s in range(count):
            square = jnp.zeros((block_rows, 1), f32)
            for c in range(tps):
                part = land_x[c, s].astype(f32)
                square = square + jnp.sum(part * part, axis=1, keepdims=True)
            scales[s * block_rows : (s + 1) * block_rows, :] = jnp.broadcast_to(
                lax.rsqrt(square / (tps * columns) + epsilon), (block_rows, 128)
            )
        for c in range(tps):
            pile = [[] for _ in range(local)]
            for s in range(count):
                scale = scales[s * block_rows : (s + 1) * block_rows, :1]
                scaled = land_x[c, s].astype(f32) * scale
                for l in range(local):
                    pile[l].append(scaled[l * capacity : (l + 1) * capacity, :])
            for l in range(local):
                normed[l, :, c * columns : (c + 1) * columns] = jnp.concatenate(
                    pile[l], axis=0
                ).astype(bf16)

    tile = min(width, 256)

    def gate_up(s, first):
        def one(i, _):
            l, n = i // (width // tile), lax.rem(i, width // tile)
            base, at = pl.multiple_of(s * rows, rows), pl.multiple_of(n * tile, tile)
            x = normed[l, :, pl.ds(base, rows)]
            for m in range(2):
                w = landing[m][l, pl.ds(base, rows), pl.ds(at, tile)]
                value = jnp.dot(x, w, preferred_element_type=f32)
                if not first:
                    value = value + sums[m, l, :, pl.ds(at, tile)]
                sums[m, l, :, pl.ds(at, tile)] = value
            return 0

        lax.fori_loop(0, local * (width // tile), one, 0)

    def activate():
        def one(i, _):
            l, n = i // (width // tile), lax.rem(i, width // tile)
            at = pl.multiple_of(n * tile, tile)
            value = jax.nn.silu(sums[0, l, :, pl.ds(at, tile)]) * sums[1, l, :, pl.ds(at, tile)]
            hidden[l, :, pl.ds(at, tile)] = value.astype(bf16)
            return 0

        lax.fori_loop(0, local * (width // tile), one, 0)

    def part_copy(s, i, giver):
        l, at = cut(i)
        col = pl.ds(pl.multiple_of(giver * share + at, piece), piece)
        return remote(
            partial.at[s, l, :, col], summing.at[t, l, :, col], part_send.at[s, i, giver],
            part_recv.at[t, i, giver], "tp", s,
        )

    def part_here(peer, i, giver):
        l, at = cut(i)
        col = pl.ds(pl.multiple_of(giver * share + at, piece), piece)
        ref = summing.at[peer, l, :, col]
        return remote(ref, ref, part_send.at[0, i, giver], part_recv.at[peer, i, giver], "tp", peer)

    def down_piece(s, i):
        l, at = cut(i)
        for giver in range(groups):
            base = pl.multiple_of(s * rows + giver * share + at, piece)
            w = down_o[l, pl.ds(base, piece), :]
            value = lax.dot_general(
                hidden[l], w, (((1,), (1,)), ((), ())), preferred_element_type=f32
            ).astype(bf16)
            col = pl.ds(pl.multiple_of(giver * share + at, piece), piece)

            @pl.when(s == t)
            def _():
                summing[t, l, :, col] = value

            @pl.when(s != t)
            def _():
                partial[s, l, :, col] = value
                part_copy(s, i, giver).start()

    def returning(j):
        return remote(send_ret.at[j], land_ret.at[z], ret_send.at[j], ret_recv.at[z], "fs", j)

    def returned(s):
        return remote(send_ret.at[s], land_ret.at[s], ret_send.at[s], ret_recv.at[s], "fs", s)

    def give_back():
        def await_part(i, _):
            for other in range(1, tps):
                for giver in range(groups):
                    part_here(lax.rem(t + other, tps), i, giver).wait_recv()
            return 0

        lax.fori_loop(0, pieces, await_part, 0)
        whole = []
        for l in range(local):
            value = summing[0, l].astype(f32)
            for c in range(1, tps):
                value = value + summing[c, l].astype(f32)
            whole.append(value)
        for j in range(count):
            block = jnp.concatenate(
                [value[j * capacity : (j + 1) * capacity, :] for value in whole], axis=0
            ).astype(bf16)

            @pl.when(z == j)
            def _():
                land_ret[j] = block

            @pl.when(z != j)
            def _():
                send_ret[j] = block
                returning(j).start()

    sends = [(r, m, None) for r in range(count - 1) for m in (0, 1)]
    keeps = [(None, m, g) for m in (0, 1) for g in range(groups)]
    late = [(r, 2, None) for r in range(count - 1)] + [(None, 2, g) for g in range(groups)]
    units = sends + keeps + late
    slots = raw.shape[0]

    def unit_load(n):
        r, m, g = units[n]
        if g is None:
            return load(m, ranked(r), mine, n % slots)
        return load(m, z, g * share, n % slots)

    def send_unit(r, m):
        j = ranked(r)

        def go(i, _):
            l, at = cut(i)
            src = stage.at[r, m, l, pl.ds(at, piece), :]
            for way in (0, 1):
                @pl.when(j > z if way == 0 else j < z)
                def _():
                    start_hop(
                        way, src, send_sem.at[r, m, i], m, i, real(way, z), real(way, z),
                        real(way, j),
                    )
            return 0

        lax.fori_loop(0, pieces, go, 0)

    def do_unit(n):
        r, m, g = units[n]
        if n + slots - 1 < len(units):
            unit_load(n + slots - 1).start()
        unit_load(n).wait()
        if g is None:
            def put(l, at, value):
                stage[r, m, l, pl.ds(at, piece), :] = value

            fold(m, n % slots, mine, put)
        else:
            def put(l, at, value):
                base = pl.multiple_of(z * rows + g * share + at, piece)
                landing[m][l, pl.ds(base, piece), :] = value

            fold(m, n % slots, g * share, put)

    for n in range(slots - 1):
        unit_load(n).start()
    gain_rows = jnp.transpose(gains[...])
    for q in range(rows // 128):
        gain_col[q * 128 : (q + 1) * 128, :] = jnp.broadcast_to(gain_rows[:, q : q + 1], (128, 128))
    pack()
    pl.semaphore_wait(barrier, count - 1 + groups - 1 + tps - 1)
    elsewhere(lambda j: dispatching(j).start())
    for n in range(len(sends)):
        do_unit(n)
        send_unit(*units[n][:2])

    land_x[t, z] = send_x[z]
    for other in range(1, tps):
        spreading(z, other).start()

    def forward(s):
        dispatched(s).wait_recv()
        for other in range(1, tps):
            spreading(s, other).start()

    elsewhere(forward)
    for n in range(len(sends), len(units)):
        do_unit(n)
    for other in range(1, tps):
        for s in range(count):
            spread(s, lax.rem(t + other, tps)).wait_recv()
    normalise()
    gate_up(z, True)

    def take_piece(way, m, item, i):
        k = real(way, z)
        l, at = cut(i)

        @pl.when(item < k * (count - k))
        def _():
            s = k - 1 - item // (count - k)
            dd = count - 1 - lax.rem(item, count - k)
            source = real(way, s)

            def awaited(ref):
                remote(
                    ref, ref, send_sem.at[0, m, i], recv_sem.at[way, item, m, i], "fs", source
                ).wait_recv()

            @pl.when(dd == k)
            def _():
                awaited(spot(m, l, at, source, y))
                for other in range(1, groups):
                    passing(source, m, i, other).start()

            @pl.when(dd > k)
            def _():
                slot = (k - 1 - s) * (count - 1 - k) + (count - 1 - dd)
                ref = transit.at[way, slot, m, l, pl.ds(at, piece), :]
                awaited(ref)
                start_hop(way, ref, relay_sem.at[way, slot, m, i], m, i, k, s, dd)

    def settled(way, item, body):
        k = real(way, z)
        kept = jnp.maximum(item, 0)
        s = k - 1 - kept // (count - k)
        dd = count - 1 - lax.rem(kept, count - k)

        @pl.when((item >= 0) & (item < k * (count - k)) & (dd == k))
        def _():
            body(real(way, s))

    most = max(k * (count - k) for k in range(count))

    def await_pass(s, m, i):
        for other in range(1, groups):
            arriving(s, m, i, other).wait_recv()

    def early_block(s):
        def one(i, _):
            for m in (0, 1):
                await_pass(s, m, i)
            return 0

        lax.fori_loop(0, pieces, one, 0)
        gate_up(s, False)

    def early(n, _):
        for m in (0, 1):
            def one(i, _):
                for way in (0, 1):
                    take_piece(way, m, n, i)
                return 0

            lax.fori_loop(0, pieces, one, 0)
            if m == 0:
                for way in (0, 1):
                    settled(way, n - 1, early_block)

        @pl.when(n == min(1, most - 1))
        def _():
            for r in range(count - 1):
                send_unit(r, 2)
        return 0

    lax.fori_loop(0, most + 1, early, 0)
    activate()

    def own_down(i, _):
        down_piece(z, i)
        return 0

    lax.fori_loop(0, pieces, own_down, 0)

    lag, wait_for = 2, 4

    def later(p, _):
        n, i = p // pieces, lax.rem(p, pieces)
        for way in (0, 1):
            take_piece(way, 2, n, i)
        q = p - lag
        before = jnp.maximum(q, 0)

        def work(s):
            j = lax.rem(before, pieces)
            await_pass(s, 2, j)
            down_piece(s, j)

        for way in (0, 1):
            settled(way, jnp.where(q >= 0, before // pieces, -1), work)

        @pl.when((p == 1) & (z == t))
        def _():
            give_back()

        q = p - wait_for
        done = jnp.maximum(q, 0)

        def close(s):
            @pl.when((s == t) & (lax.rem(done, pieces) == pieces - 1))
            def _():
                give_back()

        for way in (0, 1):
            settled(way, jnp.where(q >= 0, done // pieces, -1), close)
        return 0

    lax.fori_loop(0, most * pieces + wait_for, later, 0)

    def sent(ref, sem):
        remote(ref, ref, sem, recv_sem.at[0, 0, 0, 0], "grp", lax.rem(y + 1, groups)).wait_send()

    def drain(i, _):
        l, at = cut(i)
        for m in range(3):
            for r in range(count - 1):
                sent(stage.at[r, m, l, pl.ds(at, piece), :], send_sem.at[r, m, i])

                def passed(s):
                    for other in range(1, groups):
                        passing(s, m, i, other).wait_send()

                passed(ranked(r))
            for slot in range(transit.shape[1]):
                for way in (0, 1):
                    @pl.when(slot < z * (count - 1 - z))
                    def _():
                        sent(
                            transit.at[way, slot, m, l, pl.ds(at, piece), :],
                            relay_sem.at[way, slot, m, i],
                        )
        for s in range(count):
            @pl.when(s != t)
            def _():
                for giver in range(groups):
                    part_copy(s, i, giver).wait_send()
        return 0

    lax.fori_loop(0, pieces, drain, 0)
    elsewhere(lambda j: dispatching(j).wait_send())
    for other in range(1, tps):
        for s in range(count):
            spreading(s, other).wait_send()

    elsewhere(lambda s: returned(s).wait_recv())
    back = land_ret[...].reshape(experts * capacity, columns)
    over = (((0,), (0,)), ((), ()))
    value = lax.dot_general(combine_w[0], back, over, preferred_element_type=f32)
    value = value + lax.dot_general(combine_w[1], back, over, preferred_element_type=f32)
    mixed_o[...] = value.astype(bf16)
    elsewhere(lambda j: returning(j).wait_send())


def writer_kernel(parts, *refs):
    ins, outs, sem = refs[:4], refs[4:8], refs[8]
    local, high = ins[0].shape[:2]
    step = high // parts

    def copy(k, l, i):
        at = pl.ds(i * step, step)
        return pltpu.make_async_copy(ins[k].at[l, at, :], outs[k].at[l, at, :], sem.at[k, l, i])

    small = pltpu.make_async_copy(ins[3], outs[3], sem.at[3, 0, 0])
    jobs = [copy(k, l, i) for k in range(3) for l in range(local) for i in range(parts)] + [small]
    for job in jobs:
        job.start()
    for job in jobs:
        job.wait()


def fused(tokens, routes, route_weights, norm_gain, gate_weight, up_weight, down_weight):
    groups, count, tps = (lax.axis_size(axis) for axis in ("grp", "fs", "tp"))
    experts, rows, width = gate_weight.shape
    local, own_tokens, columns = experts // count, *tokens.shape
    capacity = own_tokens * 5 // 16
    share = rows // groups
    parts = max(1, share // 128)
    pieces = local * parts
    tall = count * capacity
    dims = (groups, count, tps, local, rows, width, parts, experts, capacity)
    shape = (local, count * rows, width)
    slots = max(1, max(k * (count - 1 - k) for k in range(count)))
    items = max(k * (count - k) for k in range(count))
    bf16, f32, sem = jnp.bfloat16, jnp.float32, pltpu.SemaphoreType.DMA
    vmem, anywhere = pl.BlockSpec(memory_space=pltpu.VMEM), pl.BlockSpec(memory_space=pl.ANY)
    block = (local * capacity, columns)
    gate, up, down, mixed, _ = pl.pallas_call(
        functools.partial(fused_kernel, dims),
        out_shape=[pltpu.VMEM(shape, bf16)] * 3
        + [pltpu.VMEM(tokens.shape, bf16)]
        + [jax.ShapeDtypeStruct((2, slots, 3, local, share, width), bf16)],
        in_specs=[vmem] * 4 + [anywhere] * 3,
        out_specs=[vmem] * 4 + [anywhere],
        scratch_shapes=[
            pltpu.VMEM((3, local, share, width), f32),
            pltpu.VMEM((count - 1, 3, local, share, width), bf16),
            pltpu.VMEM((rows, 128), f32),
            pltpu.VMEM((experts * capacity, 128), f32),
            pltpu.VMEM((count,) + block, bf16),
            pltpu.VMEM((tps, count) + block, bf16),
            pltpu.VMEM((local, tall, tps * columns), bf16),
            pltpu.VMEM((2, local, tall, width), f32),
            pltpu.VMEM((local, tall, width), bf16),
            pltpu.VMEM((count, local, tall, columns), bf16),
            pltpu.VMEM((tps, local, tall, columns), bf16),
            pltpu.VMEM((2, experts * capacity, own_tokens), bf16),
            pltpu.VMEM((count,) + block, bf16),
            pltpu.VMEM((count,) + block, bf16),
            sem((3,)), sem((count - 1, 3, pieces)), sem((2, items, 3, pieces)),
            sem((2, slots, 3, pieces)),
            sem((count, 3, pieces, groups - 1)), sem((count, 3, pieces, groups - 1)),
            sem((count,)), sem((count,)), sem((tps, count)), sem((tps, count)),
            sem((count, pieces, groups)), sem((tps, pieces, groups)), sem((count,)), sem((count,)),
        ],
        compiler_params=pltpu.CompilerParams(
            collective_id=1, has_side_effects=True, vmem_limit_bytes=38 * 1024 * 1024
        ),
    )(
        tokens, routes.T, route_weights.T, norm_gain.reshape(rows // 128, 128),
        gate_weight, up_weight, down_weight,
    )
    parts = max(1, shape[1] // 512)
    return pl.pallas_call(
        functools.partial(writer_kernel, parts),
        out_shape=[jax.ShapeDtypeStruct(shape, bf16)] * 3
        + [jax.ShapeDtypeStruct(tokens.shape, bf16)],
        in_specs=[vmem] * 4,
        out_specs=[anywhere] * 4,
        scratch_shapes=[sem((4, local, parts))],
        compiler_params=pltpu.CompilerParams(vmem_limit_bytes=1024 * 1024),
    )(gate, up, down, mixed)


def on_device(tokens, routes, route_weights, norm_gain, gate_weight, up_weight, down_weight):
    groups, count, tps = (lax.axis_size(axis) for axis in ("grp", "fs", "tp"))
    experts, rows, width = gate_weight.shape
    own_tokens, columns = tokens.shape
    capacity = own_tokens * 5 // 16
    fits = (
        groups > 1 and 1 < count <= 8 and experts % count == 0 and rows == columns
        and count == tps and rows % (128 * groups) == 0 and width % 128 == 0
        and capacity % 8 == 0 and (experts // count * capacity) % 16 == 0
        and 6 * experts // count * count * rows * width <= 24 * 1024 * 1024
    )
    body = fused if fits else layered
    return tuple(
        body(tokens, routes, route_weights, norm_gain, gate_weight, up_weight, down_weight)
    )


def solution(mesh):
    in_specs = (
        P(("grp", "fs"), "tp"),
        P(("grp", "fs"), None),
        P(("grp", "fs"), None),
        P("fs"),
        P(None, "fs", "tp"),
        P(None, "fs", "tp"),
        P(None, "fs", "tp"),
    )
    out_specs = (
        P("fs", "grp", "tp"),
        P("fs", "grp", "tp"),
        P("fs", "grp", "tp"),
        P(("grp", "fs"), "tp"),
    )
    return jax.shard_map(
        on_device, mesh=mesh, in_specs=in_specs, out_specs=out_specs, check_vma=False
    )
```

```python
import functools

import jax
import jax.numpy as jnp
from jax import lax
from jax.experimental import pallas as pl
from jax.experimental.pallas import tpu as pltpu
from jax.sharding import PartitionSpec as P

epsilon = 1e-06
MESH = pl.DeviceIdType.MESH


def expert_slots(routes, experts, capacity):
    row_count = routes.shape[0] * routes.shape[1]
    flat_routes = routes.reshape(row_count)
    onehot = (flat_routes[:, None] == jnp.arange(experts, dtype=jnp.int32)[None, :]).astype(
        jnp.int32
    )
    earlier = jnp.cumsum(onehot, axis=0) - onehot
    position = jnp.sum(earlier * onehot, axis=1)
    return (flat_routes * capacity + position).reshape(routes.shape)


def dispatch(normed, slots, experts, capacity, copies, local_count):
    col_width = normed.shape[1]
    slot_ids = jnp.arange(experts * capacity, dtype=jnp.int32)
    select = jnp.any(slot_ids[:, None, None] == slots[None, :, :], axis=2).astype(jnp.bfloat16)
    packed = jnp.dot(select, normed, preferred_element_type=jnp.float32).astype(jnp.bfloat16)
    packed = jnp.broadcast_to(
        packed.reshape(experts, 1, capacity, col_width), (experts, copies, capacity, col_width)
    )
    return packed.reshape(experts * copies // local_count, local_count, capacity, col_width)


def combine(returned, slots, route_weights, experts, copies):
    capacity, col_width = (returned.shape[2], returned.shape[3])
    summed_up = jnp.sum(
        returned.reshape(experts, copies, capacity, col_width), axis=1, dtype=jnp.float32
    )
    selected = summed_up.reshape(experts * capacity, col_width)[slots]
    return jnp.sum(route_weights[:, :, None] * selected, axis=1)


def exchange_kernel(
    dims, gains, gate_w, up_w, down_w, gate_o, up_o, down_o,
    raw, stage, load_sem, send_sem, recv_sem, pass_send, pass_recv,
):
    groups, count, local, copies, rows, width, parts = dims
    weights, landing = (gate_w, up_w, down_w), (gate_o, up_o, down_o)
    y, z = lax.axis_index("grp"), lax.axis_index("fs")
    share = rows // groups
    piece = share // parts

    barrier = pltpu.get_barrier_semaphore()

    def greet(j, _):
        @pl.when(j != z)
        def _():
            pl.semaphore_signal(barrier, inc=1, device_id={"fs": j}, device_id_type=MESH)
        return 0

    lax.fori_loop(0, count, greet, 0)
    for other in range(1, groups):
        pl.semaphore_signal(
            barrier, inc=1, device_id={"grp": lax.rem(y + other, groups)}, device_id_type=MESH
        )

    def load(m, j, first, slot):
        if copies > 1:
            expert, column = j // copies, lax.rem(j, copies) * width
            column = pl.ds(pl.multiple_of(column, 128), width)
        else:
            expert, column = j * local, slice(None)
        return pltpu.make_async_copy(
            weights[m].at[pl.ds(expert, local), pl.ds(first, share), column],
            raw.at[slot], load_sem.at[slot],
        )

    def fold(m, slot, first, put):
        def one(i, _):
            l, q = i // parts, lax.rem(i, parts)
            at = pl.multiple_of(q * piece, piece)
            scaled = raw[slot, l, pl.ds(at, piece), :]
            if m < 2:
                scaled = scaled * gains[pl.ds(pl.multiple_of(first + at, piece), piece), :1]
            put(l, at, scaled.astype(jnp.bfloat16))
            return 0

        lax.fori_loop(0, local * parts, one, 0)

    def sending(j, m, i):
        l, q = i // parts, lax.rem(i, parts)
        at = pl.multiple_of(q * piece, piece)
        base = pl.multiple_of(z * rows + y * share + at, piece)
        return pltpu.make_async_remote_copy(
            src_ref=stage.at[j, m, l, pl.ds(at, piece), :],
            dst_ref=landing[m].at[l, pl.ds(base, piece), :],
            send_sem=send_sem.at[j, m, i],
            recv_sem=recv_sem.at[z, m, i],
            device_id={"fs": j}, device_id_type=MESH,
        )

    def passing(s, m, i, other):
        l, q = i // parts, lax.rem(i, parts)
        base = pl.multiple_of(s * rows + y * share + q * piece, piece)
        spot = landing[m].at[l, pl.ds(base, piece), :]
        return pltpu.make_async_remote_copy(
            src_ref=spot, dst_ref=spot,
            send_sem=pass_send.at[s, m, i, other - 1],
            recv_sem=pass_recv.at[s, m, i, other - 1],
            device_id={"grp": lax.rem(y + other, groups)}, device_id_type=MESH,
        )

    def arriving(s, m, i, other):
        l, q = i // parts, lax.rem(i, parts)
        giver = lax.rem(y + groups - other, groups)
        base = pl.multiple_of(s * rows + giver * share + q * piece, piece)
        spot = landing[m].at[l, pl.ds(base, piece), :]
        return pltpu.make_async_remote_copy(
            src_ref=spot, dst_ref=spot,
            send_sem=pass_send.at[s, m, i, other - 1],
            recv_sem=pass_recv.at[s, m, i, other - 1],
            device_id={"grp": giver}, device_id_type=MESH,
        )

    def landed(s, m, i):
        l, q = i // parts, lax.rem(i, parts)
        base = pl.multiple_of(s * rows + y * share + q * piece, piece)
        return pltpu.make_async_remote_copy(
            src_ref=landing[m].at[l, pl.ds(base, piece), :],
            dst_ref=landing[m].at[l, pl.ds(base, piece), :],
            send_sem=send_sem.at[s, m, i],
            recv_sem=recv_sem.at[s, m, i],
            device_id={"fs": s}, device_id_type=MESH,
        )

    mine = pl.multiple_of(y * share, share)
    pieces = local * parts

    def neighbours(body):
        def step(d, _):
            for j, there in ((z + d, z + d < count), (z - d, z - d >= 0)):
                @pl.when(there)
                def _():
                    body(j)
            return 0

        lax.fori_loop(1, count, step, 0)

    def send_phase(phase):
        def to(j):
            for m in phase:
                load(m, j, mine, m % 2).start()
            for m in phase:
                load(m, j, mine, m % 2).wait()

                def put(l, at, value):
                    stage[j, m, l, pl.ds(at, piece), :] = value

                fold(m, m % 2, mine, put)
            for m in phase:
                def go(i, _):
                    sending(j, m, i).start()
                    return 0

                lax.fori_loop(0, pieces, go, 0)

        neighbours(to)

    pl.semaphore_wait(barrier, count - 1 + groups - 1)
    send_phase((0, 1))
    send_phase((2,))

    for m in range(3):
        for g in range(groups):
            load(m, z, g * share, g % 2).start()
            load(m, z, g * share, g % 2).wait()

            def put(l, at, value):
                base = pl.multiple_of(z * rows + g * share + at, piece)
                landing[m][l, pl.ds(base, piece), :] = value

            fold(m, g % 2, g * share, put)

    def pass_phase(phase):
        def take(s):
            for m in phase:
                def one(i, _):
                    landed(s, m, i).wait_recv()
                    for other in range(1, groups):
                        passing(s, m, i, other).start()
                    return 0

                lax.fori_loop(0, pieces, one, 0)

        neighbours(take)

    pass_phase((0, 1))
    pass_phase((2,))

    def finish(s):
        for m in range(3):
            def one(i, _):
                for other in range(1, groups):
                    arriving(s, m, i, other).wait_recv()
                    passing(s, m, i, other).wait_send()
                sending(s, m, i).wait_send()
                return 0

            lax.fori_loop(0, pieces, one, 0)

    neighbours(finish)


def relay_kernel(
    dims, gains, gate_w, up_w, down_w, gate_o, up_o, down_o,
    raw, stage, transit, load_sem, send_sem, recv_sem, relay_sem, pass_send, pass_recv,
):
    groups, count, local, copies, rows, width, parts = dims
    weights, landing = (gate_w, up_w, down_w), (gate_o, up_o, down_o)
    y, z = lax.axis_index("grp"), lax.axis_index("fs")
    share = rows // groups
    piece = share // parts
    pieces = local * parts
    mine = pl.multiple_of(y * share, share)

    def real(way, place):
        return place if way == 0 else count - 1 - place

    barrier = pltpu.get_barrier_semaphore()
    for j, there in ((z + 1, z + 1 < count), (z - 1, z >= 1)):
        @pl.when(there)
        def _():
            pl.semaphore_signal(barrier, inc=1, device_id={"fs": j}, device_id_type=MESH)
    for other in range(1, groups):
        pl.semaphore_signal(
            barrier, inc=1, device_id={"grp": lax.rem(y + other, groups)}, device_id_type=MESH
        )

    def load(m, j, first, slot):
        if copies > 1:
            expert, column = j // copies, lax.rem(j, copies) * width
            column = pl.ds(pl.multiple_of(column, 128), width)
        else:
            expert, column = j * local, slice(None)
        return pltpu.make_async_copy(
            weights[m].at[pl.ds(expert, local), pl.ds(first, share), column],
            raw.at[slot], load_sem.at[slot],
        )

    def cut(i):
        return i // parts, pl.multiple_of(lax.rem(i, parts) * piece, piece)

    def fold(m, slot, first, put):
        def one(i, _):
            l, at = cut(i)
            scaled = raw[slot, l, pl.ds(at, piece), :]
            if m < 2:
                scaled = scaled * gains[pl.ds(pl.multiple_of(first + at, piece), piece), :1]
            put(l, at, scaled.astype(jnp.bfloat16))
            return 0

        lax.fori_loop(0, pieces, one, 0)

    def spot(m, l, at, source, giver):
        base = pl.multiple_of(source * rows + giver * share + at, piece)
        return landing[m].at[l, pl.ds(base, piece), :]

    def hop(way, src, sem, m, i, k, s, dd, final):
        l, at = cut(i)
        if final:
            dst = spot(m, l, at, real(way, s), y)
        else:
            slot = (k - s) * (count - 2 - k) + (count - 1 - dd)
            dst = transit.at[way, slot, m, l, pl.ds(at, piece), :]
        place = (k - s) * (count - 1 - k) + (count - 1 - dd)
        return pltpu.make_async_remote_copy(
            src_ref=src, dst_ref=dst, send_sem=sem,
            recv_sem=recv_sem.at[way, place, m, i],
            device_id={"fs": real(way, k + 1)}, device_id_type=MESH,
        )

    def start_hop(way, src, sem, m, i, k, s, dd):
        @pl.when(dd == k + 1)
        def _():
            hop(way, src, sem, m, i, k, s, dd, True).start()

        @pl.when(dd > k + 1)
        def _():
            hop(way, src, sem, m, i, k, s, dd, False).start()

    def passing(s, m, i, other):
        l, at = cut(i)
        ref = spot(m, l, at, s, y)
        return pltpu.make_async_remote_copy(
            src_ref=ref, dst_ref=ref,
            send_sem=pass_send.at[s, m, i, other - 1],
            recv_sem=pass_recv.at[s, m, i, other - 1],
            device_id={"grp": lax.rem(y + other, groups)}, device_id_type=MESH,
        )

    def arriving(s, m, i, other):
        l, at = cut(i)
        giver = lax.rem(y + groups - other, groups)
        ref = spot(m, l, at, s, giver)
        return pltpu.make_async_remote_copy(
            src_ref=ref, dst_ref=ref,
            send_sem=pass_send.at[s, m, i, other - 1],
            recv_sem=pass_recv.at[s, m, i, other - 1],
            device_id={"grp": giver}, device_id_type=MESH,
        )

    def send_phase(phase):
        def step(d, _):
            for way in (0, 1):
                k = real(way, z)
                dd = count - d
                j = real(way, dd)

                @pl.when(dd > k)
                def _():
                    for m in phase:
                        load(m, j, mine, m).start()
                    for m in phase:
                        load(m, j, mine, m).wait()

                        def put(l, at, value):
                            stage[j, m, l, pl.ds(at, piece), :] = value

                        fold(m, m, mine, put)

                        def go(i, _):
                            l, at = cut(i)
                            src = stage.at[j, m, l, pl.ds(at, piece), :]
                            start_hop(way, src, send_sem.at[j, m, i], m, i, k, k, dd)
                            return 0

                        lax.fori_loop(0, pieces, go, 0)
            return 0

        lax.fori_loop(1, count, step, 0)

    def own_block():
        for m in range(3):
            for g in range(groups):
                load(m, z, g * share, g % 2).start()
                load(m, z, g * share, g % 2).wait()

                def put(l, at, value):
                    stage[z, m, l, pl.ds(at, piece), :] = value

                fold(m, g % 2, g * share, put)
                base = pl.multiple_of(z * rows + g * share, share)
                keep = pltpu.make_async_copy(
                    stage.at[z, m], landing[m].at[:, pl.ds(base, share), :], load_sem.at[g % 2]
                )
                keep.start()
                keep.wait()

    def take_phase(phase):
        most = max(k * (count - k) for k in range(count))

        def take(item, _):
            for m in phase:
                def one(i, _):
                    l, at = cut(i)
                    for way in (0, 1):
                        take_piece(way, m, item, i, l, at)
                    return 0

                lax.fori_loop(0, pieces, one, 0)
            return 0

        lax.fori_loop(0, most, take, 0)

    def take_piece(way, m, item, i, l, at):
        k = real(way, z)

        @pl.when(item < k * (count - k))
        def _():
            s = k - 1 - item // (count - k)
            dd = count - 1 - lax.rem(item, count - k)
            source = real(way, s)

            def awaited(ref):
                pltpu.make_async_remote_copy(
                    src_ref=ref, dst_ref=ref, send_sem=send_sem.at[source, m, i],
                    recv_sem=recv_sem.at[way, item, m, i],
                    device_id={"fs": source}, device_id_type=MESH,
                ).wait_recv()

            @pl.when(dd == k)
            def _():
                awaited(spot(m, l, at, source, y))
                for other in range(1, groups):
                    passing(source, m, i, other).start()

            @pl.when(dd > k)
            def _():
                slot = (k - 1 - s) * (count - 1 - k) + (count - 1 - dd)
                ref = transit.at[way, slot, m, l, pl.ds(at, piece), :]
                awaited(ref)
                start_hop(way, ref, relay_sem.at[way, slot, m, i], m, i, k, s, dd)

    def sent(ref, sem):
        pltpu.make_async_remote_copy(
            src_ref=ref, dst_ref=ref, send_sem=sem, recv_sem=recv_sem.at[0, 0, 0, 0],
            device_id={"grp": lax.rem(y + 1, groups)}, device_id_type=MESH,
        ).wait_send()

    def finish():
        def block(t, _):
            s, i = t // pieces, lax.rem(t, pieces)
            l, at = cut(i)

            @pl.when(s != z)
            def _():
                for m in range(3):
                    for other in range(1, groups):
                        arriving(s, m, i, other).wait_recv()
                        passing(s, m, i, other).wait_send()
                    sent(stage.at[s, m, l, pl.ds(at, piece), :], send_sem.at[s, m, i])
            return 0

        lax.fori_loop(0, count * pieces, block, 0)

        def passed(t, _):
            slot, i = t // pieces, lax.rem(t, pieces)
            l, at = cut(i)
            for way in (0, 1):
                @pl.when(slot < z * (count - 1 - z))
                def _():
                    for m in range(3):
                        sent(
                            transit.at[way, slot, m, l, pl.ds(at, piece), :],
                            relay_sem.at[way, slot, m, i],
                        )
            return 0

        lax.fori_loop(0, transit.shape[1] * pieces, passed, 0)

    ends = (z == 0).astype(jnp.int32) + (z == count - 1).astype(jnp.int32)
    pl.semaphore_wait(barrier, 2 - ends + groups - 1)
    send_phase((0, 1, 2))
    own_block()
    take_phase((0, 1, 2))
    finish()


def exchange(norm_gain, gate_weight, up_weight, down_weight, groups, count, copies, local):
    experts, rows, columns = gate_weight.shape
    width = columns // copies
    share = rows // groups
    parts = max(1, share // 128)
    gains = jnp.broadcast_to(norm_gain[:, None], (rows, 128))
    shape = (local, count * rows, width)
    dims = (groups, count, local, copies, rows, width, parts)
    pieces = local * parts
    relaying = 1 < count <= 8 and groups > 1
    common = [
        pltpu.VMEM((3, local, share, width), jnp.float32),
        pltpu.VMEM((count, 3, local, share, width), jnp.bfloat16),
    ]
    sem = pltpu.SemaphoreType.DMA
    passes = [sem((count, 3, pieces, max(1, groups - 1)))] * 2
    if relaying:
        slots = max(1, max(k * (count - 1 - k) for k in range(count)))
        items = max(k * (count - k) for k in range(count))
        scratch = common + [
            pltpu.VMEM((2, slots, 3, local, share, width), jnp.bfloat16),
            sem((3,)), sem((count, 3, pieces)), sem((2, items, 3, pieces)),
            sem((2, slots, 3, pieces)),
        ] + passes
    else:
        scratch = common + [sem((2,))] + [sem((count, 3, pieces))] * 2 + passes
    return pl.pallas_call(
        functools.partial(relay_kernel if relaying else exchange_kernel, dims),
        out_shape=[jax.ShapeDtypeStruct(shape, jnp.bfloat16)] * 3,
        in_specs=[pl.BlockSpec(memory_space=pltpu.VMEM)]
        + [pl.BlockSpec(memory_space=pl.ANY)] * 3,
        out_specs=[pl.BlockSpec(memory_space=pl.ANY if relaying else pltpu.VMEM)] * 3,
        scratch_shapes=scratch,
        compiler_params=pltpu.CompilerParams(
            collective_id=0, has_side_effects=True, vmem_limit_bytes=60 * 1024 * 1024
        ),
    )(gains, gate_weight, up_weight, down_weight)


def layered(tokens, routes, route_weights, norm_gain, gate_weight, up_weight, down_weight):
    groups = lax.axis_size("grp")
    fs_count = lax.axis_size("fs")
    tp_count = lax.axis_size("tp")
    experts = gate_weight.shape[0]
    copies = max(1, fs_count // experts)
    local_count = max(1, experts // fs_count)
    capacity = tokens.shape[0] * 5 // 16

    gate_new, up_new, down_new = exchange(
        norm_gain, gate_weight, up_weight, down_weight, groups, fs_count, copies, local_count
    )
    slots = expert_slots(routes, experts, capacity)
    whole = lax.all_gather(tokens, "tp", axis=1, tiled=True)
    widened = whole.astype(jnp.float32)
    row_scale = lax.rsqrt(jnp.mean(widened * widened, axis=1, keepdims=True) + epsilon)
    normed = (widened * row_scale).astype(jnp.bfloat16)
    outgoing = dispatch(normed, slots, experts, capacity, copies, local_count)
    arrived = lax.all_to_all(outgoing, "fs", split_axis=0, concat_axis=0, tiled=True)
    gate_sums = jnp.einsum("slcd,ldf->slcf", arrived, gate_new, preferred_element_type=jnp.float32)
    up_sums = jnp.einsum("slcd,ldf->slcf", arrived, up_new, preferred_element_type=jnp.float32)
    hidden = (jax.nn.silu(gate_sums) * up_sums).astype(jnp.bfloat16)
    partial_value = jnp.einsum(
        "slcf,ldf->slcd", hidden, down_new, preferred_element_type=jnp.float32
    ).astype(jnp.bfloat16)
    by_columns = partial_value.reshape(
        partial_value.shape[:3] + (tp_count, partial_value.shape[3] // tp_count)
    )
    exchanged = lax.all_to_all(by_columns, "tp", split_axis=3, concat_axis=3, tiled=True)
    summed_up = jnp.sum(exchanged, axis=3, dtype=jnp.float32)
    handed = lax.all_to_all(
        summed_up.astype(jnp.bfloat16), "fs", split_axis=0, concat_axis=0, tiled=True
    ).astype(summed_up.dtype)
    combined = combine(handed, slots, route_weights, experts, copies)
    return (gate_new, up_new, down_new, combined.astype(jnp.bfloat16))


def far_first(count):
    table = []
    for z in range(count):
        right = [j for j in range(count - 1, z, -1)]
        left = [j for j in range(z)]
        ways, order = sorted((right, left), key=len, reverse=True), []
        for d in range(count):
            order += [way[d] for way in ways if d < len(way)]
        table.append(order)
    return table


def fused_kernel(
    dims, tokens, routes, route_weights, gains, gate_w, up_w, down_w,
    gate_o, up_o, down_o, mixed_o, transit,
    raw, stage, gain_col, scales, send_x, land_x, normed, sums, hidden, partial, across, summing, combine_w,
    send_ret, land_ret,
    load_sem, send_sem, recv_sem, relay_sem, pass_send, pass_recv,
    x_send, x_recv, xg_send, xg_recv, part_send, part_recv, ret_send, ret_recv,
    across_send, hid_send, hid_recv, go_sem,
):
    groups, count, tps, local, rows, width, parts, experts, capacity = dims
    weights, landing = (gate_w, up_w, down_w), (gate_o, up_o, down_o)
    y, z, t = lax.axis_index("grp"), lax.axis_index("fs"), lax.axis_index("tp")
    share = rows // groups
    piece = share // parts
    pieces = local * parts
    mine = pl.multiple_of(y * share, share)
    table = far_first(count)
    block_rows = local * capacity
    own_tokens, columns = tokens.shape
    tall = count * capacity
    f32, bf16 = jnp.float32, jnp.bfloat16

    def ranked(r):
        return sum((z == k).astype(jnp.int32) * table[k][r] for k in range(count))

    def real(way, place):
        return place if way == 0 else count - 1 - place

    def remote(src, dst, send, recv, axis, index):
        return pltpu.make_async_remote_copy(
            src_ref=src, dst_ref=dst, send_sem=send, recv_sem=recv,
            device_id={axis: index}, device_id_type=MESH,
        )

    barrier = pltpu.get_barrier_semaphore()
    for axis, me, size in (("fs", z, count), ("grp", y, groups), ("tp", t, tps)):
        for other in range(1, size):
            pl.semaphore_signal(
                barrier, inc=1, device_id={axis: lax.rem(me + other, size)}, device_id_type=MESH
            )

    def load(m, j, first, slot):
        return pltpu.make_async_copy(
            weights[m].at[pl.ds(j * local, local), pl.ds(first, share), :],
            raw.at[slot], load_sem.at[slot],
        )

    def cut(i):
        return i // parts, pl.multiple_of(lax.rem(i, parts) * piece, piece)

    def fold(m, slot, first, put):
        def one(i, _):
            l, at = cut(i)
            scaled = raw[slot, l, pl.ds(at, piece), :]
            if m < 2:
                scaled = scaled * gain_col[pl.ds(pl.multiple_of(first + at, piece), piece), :1]
            put(l, at, scaled.astype(bf16))
            return 0

        lax.fori_loop(0, pieces, one, 0)

    def spot(m, l, at, source, giver):
        base = pl.multiple_of(source * rows + giver * share + at, piece)
        return landing[m].at[l, pl.ds(base, piece), :]

    def start_hop(way, src, sem, m, i, k, s, dd):
        l, at = cut(i)
        place = (k - s) * (count - 1 - k) + (count - 1 - dd)
        recv = recv_sem.at[way, place, m, i]

        @pl.when(dd == k + 1)
        def _():
            remote(src, spot(m, l, at, real(way, s), y), sem, recv, "fs", real(way, k + 1)).start()

        @pl.when(dd > k + 1)
        def _():
            slot = (k - s) * (count - 2 - k) + (count - 1 - dd)
            dst = transit.at[way, slot, m, l, pl.ds(at, piece), :]
            remote(src, dst, sem, recv, "fs", real(way, k + 1)).start()

    def passing(s, m, i, other):
        l, at = cut(i)
        ref = spot(m, l, at, s, y)
        return remote(
            ref, ref, pass_send.at[s, m, other - 1], pass_recv.at[s, m, i, other - 1],
            "grp", lax.rem(y + other, groups),
        )

    def arriving(s, m, i, other):
        l, at = cut(i)
        giver = lax.rem(y + groups - other, groups)
        ref = spot(m, l, at, s, giver)
        return remote(
            ref, ref, pass_send.at[s, m, other - 1], pass_recv.at[s, m, i, other - 1],
            "grp", giver,
        )

    def slot_rows():
        wanted = routes[...]
        expert_ids = lax.broadcasted_iota(jnp.int32, (experts, own_tokens), 0)
        onehots = [
            (expert_ids == wanted[k : k + 1, :]).astype(f32) for k in range(wanted.shape[0])
        ]
        before = lax.broadcasted_iota(jnp.int32, (own_tokens, own_tokens), 0)
        after = lax.broadcasted_iota(jnp.int32, (own_tokens, own_tokens), 1)
        upper = (before < after).astype(bf16)
        earlier = jnp.dot(sum(onehots).astype(bf16), upper, preferred_element_type=f32)
        found = []
        for k, onehot in enumerate(onehots):
            position = jnp.sum(earlier * onehot, axis=0, keepdims=True)
            earlier = earlier + onehot
            found.append(wanted[k : k + 1, :] * capacity + position.astype(jnp.int32))
        return found

    def pack():
        found = slot_rows()
        shape = (combine_w.shape[2], own_tokens)
        slot_ids = lax.broadcasted_iota(jnp.int32, shape, 0)
        chosen, weighed = jnp.zeros(shape, f32), jnp.zeros(shape, f32)
        for k, slot in enumerate(found):
            hit = slot_ids == slot
            chosen = jnp.where(hit, 1.0, chosen)
            weighed = weighed + jnp.where(hit, route_weights[k : k + 1, :], 0.0)
        packed = jnp.dot(chosen.astype(bf16), tokens[...], preferred_element_type=f32)
        packed = packed.astype(bf16)
        for j in range(count):
            send_x[j] = packed[j * block_rows : (j + 1) * block_rows, :]
        weighed = jnp.transpose(weighed)
        high = weighed.astype(bf16)
        combine_w[0] = high
        combine_w[1] = (weighed - high.astype(f32)).astype(bf16)

    def dispatching(j):
        return remote(send_x.at[j], land_x.at[t, z], x_send.at[j], x_recv.at[z], "fs", j)

    def dispatched(s):
        return remote(send_x.at[s], land_x.at[t, s], x_send.at[s], x_recv.at[s], "fs", s)

    def spreading(s, other):
        return remote(
            land_x.at[t, s], land_x.at[t, s], xg_send.at[0], xg_recv.at[0],
            "tp", lax.rem(t + other, tps),
        )

    def spread():
        ref = land_x.at[pl.ds(0, tps - 1)]
        return remote(ref, ref, xg_send.at[0], xg_recv.at[0], "tp", lax.rem(t + 1, tps))

    def elsewhere(body):
        for other in range(1, count):
            body(lax.rem(z + other, count))

    def normalise():
        for s in range(count):
            square = jnp.zeros((block_rows, 1), f32)
            for c in range(tps):
                part = land_x[c, s].astype(f32)
                square = square + jnp.sum(part * part, axis=1, keepdims=True)
            scales[s * block_rows : (s + 1) * block_rows, :] = jnp.broadcast_to(
                lax.rsqrt(square / (tps * columns) + epsilon), (block_rows, 128)
            )
        for c in range(tps):
            pile = [[] for _ in range(local)]
            for s in range(count):
                scale = scales[s * block_rows : (s + 1) * block_rows, :1]
                scaled = land_x[c, s].astype(f32) * scale
                for l in range(local):
                    pile[l].append(scaled[l * capacity : (l + 1) * capacity, :])
            for l in range(local):
                normed[l, :, c * columns : (c + 1) * columns] = jnp.concatenate(
                    pile[l], axis=0
                ).astype(bf16)

    tile = min(width, 256)

    def gate_up(s, first):
        def one(i, _):
            l, n = i // (width // tile), lax.rem(i, width // tile)
            base, at = pl.multiple_of(s * rows, rows), pl.multiple_of(n * tile, tile)
            x = normed[l, :, pl.ds(base, rows)]
            for m in range(2):
                w = landing[m][l, pl.ds(base, rows), pl.ds(at, tile)]
                value = jnp.dot(x, w, preferred_element_type=f32)
                if not first:
                    value = value + sums[m, l, :, pl.ds(at, tile)]
                sums[m, l, :, pl.ds(at, tile)] = value
            return 0

        lax.fori_loop(0, local * (width // tile), one, 0)

    def activate():
        def one(i, _):
            l, n = i // (width // tile), lax.rem(i, width // tile)
            at = pl.multiple_of(n * tile, tile)
            value = jax.nn.silu(sums[0, l, :, pl.ds(at, tile)]) * sums[1, l, :, pl.ds(at, tile)]
            hidden[y, l, :, pl.ds(at, tile)] = value.astype(bf16)
            return 0

        lax.fori_loop(0, local * (width // tile), one, 0)

    half = count // 2
    most = max(k * (count - k) for k in range(count))

    def comes_last(s):
        place = jnp.where(z > s, z, count - 1 - z)
        origin = jnp.where(z > s, s, count - 1 - s)
        arrival = (place - 1 - origin) * (count - place) + (count - 1 - place)
        return (z != s) & (arrival == most - 1)

    last = comes_last(t)

    def feature(giver, at):
        return pl.ds(pl.multiple_of(giver * share + at, piece), piece)

    def lending(other):
        return pltpu.make_async_remote_copy(
            src_ref=hidden.at[y, local - 1], dst_ref=hidden.at[y, local - 1],
            send_sem=hid_send.at[other], recv_sem=hid_recv.at[y], device_id={"grp": lax.rem(y + other, groups)},
            device_id_type=MESH,
        )

    def lent(other):
        giver = lax.rem(y + other, groups)
        ref = hidden.at[giver, local - 1]
        return remote(ref, ref, hid_send.at[other], hid_recv.at[giver], "grp", giver)

    def part_copy(s, i, giver):
        l, at = cut(i)
        col = feature(giver, at)
        return remote(
            partial.at[s, l, :, col], summing.at[t, l, :, col], part_send.at[s, i, giver],
            part_recv.at[t, i, giver], "tp", s,
        )

    final = pieces - 1

    def part_across(way, s, other):
        l, at = cut(final)
        return pltpu.make_async_remote_copy(
            src_ref=across.at[way, other - 1],
            dst_ref=summing.at[t, l, :, feature(y, at)],
            send_sem=across_send.at[way, other - 1], recv_sem=part_recv.at[t, final, y],
            device_id={"grp": lax.rem(y + other, groups), "tp": s}, device_id_type=MESH,
        )

    def part_here(peer, i, giver):
        l, at = cut(i)
        ref = summing.at[peer, l, :, feature(giver, at)]
        return remote(ref, ref, part_send.at[0, i, giver], part_recv.at[peer, i, giver], "tp", peer)

    def down_rows(group, s, i, giver):
        l, at = cut(i)
        base = pl.multiple_of(s * rows + giver * share + at, piece)
        return lax.dot_general(
            hidden[group, l], down_o[l, pl.ds(base, piece), :], (((1,), (1,)), ((), ())),
            preferred_element_type=f32,
        ).astype(bf16)

    def down_piece(s, i, givers):
        l, at = cut(i)
        for giver in givers:
            value = down_rows(y, s, i, giver)

            @pl.when(s == t)
            def _():
                summing[t, l, :, feature(giver, at)] = value

            @pl.when(s != t)
            def _():
                partial[s, l, :, feature(giver, at)] = value

        @pl.when(s != t)
        def _():
            for giver in givers:
                part_copy(s, i, giver).start()

    def down_last(way, s):
        for other in range(1, groups):
            across[way, other - 1] = down_rows(lax.rem(y + other, groups), s, final, y)
        down_piece(s, final, (y,))
        for other in range(1, groups):
            part_across(way, s, other).start()

    def close_piece(i):
        l, at = cut(i)
        for giver in range(groups):
            for other in range(1, tps):
                part_here(lax.rem(t + other, tps), i, giver).wait_recv()

            @pl.when((y != giver) & last & (i == final))
            def _():
                part_here(t, i, giver).wait_recv()

            col = feature(giver, at)
            value = summing[0, l, :, col].astype(f32)
            for peer in range(1, tps):
                value = value + summing[peer, l, :, col].astype(f32)
            sums[0, l, :, col] = value

    def returning(j):
        return remote(send_ret.at[j], land_ret.at[z], ret_send.at[j], ret_recv.at[z], "fs", j)

    def returned(s):
        return remote(send_ret.at[s], land_ret.at[s], ret_send.at[s], ret_recv.at[s], "fs", s)

    def give_back():
        for j in range(count):
            block = jnp.concatenate(
                [
                    sums[0, l, j * capacity : (j + 1) * capacity, :columns]
                    for l in range(local)
                ],
                axis=0,
            ).astype(bf16)

            @pl.when(z == j)
            def _():
                land_ret[j] = block

            @pl.when(z != j)
            def _():
                send_ret[j] = block
        for r in range(count - 1):
            returning(ranked(r)).start()

    sends = [(r, m, None) for r in range(count - 1) for m in (0, 1)]
    keeps = [(None, m, g) for m in (0, 1) for g in range(groups)]
    late = [(r, 2, None) for r in range(count - 1)] + [(None, 2, g) for g in range(groups)]
    units = sends + keeps + late
    slots = raw.shape[0]

    def unit_load(n):
        r, m, g = units[n]
        if g is None:
            return load(m, ranked(r), mine, n % slots)
        return load(m, z, g * share, n % slots)

    def send_unit(r, m):
        j = ranked(r)

        def go(i, _):
            l, at = cut(i)
            src = stage.at[r, m, l, pl.ds(at, piece), :]
            for way in (0, 1):
                @pl.when(j > z if way == 0 else j < z)
                def _():
                    start_hop(
                        way, src, send_sem.at[r], m, i, real(way, z), real(way, z),
                        real(way, j),
                    )
            return 0

        lax.fori_loop(0, pieces, go, 0)

    def do_unit(n):
        r, m, g = units[n]
        if n + slots - 1 < len(units):
            unit_load(n + slots - 1).start()
        unit_load(n).wait()
        if g is None:
            def put(l, at, value):
                stage[r, m, l, pl.ds(at, piece), :] = value

            fold(m, n % slots, mine, put)
        else:
            def put(l, at, value):
                base = pl.multiple_of(z * rows + g * share + at, piece)
                landing[m][l, pl.ds(base, piece), :] = value

            fold(m, n % slots, g * share, put)

    for n in range(slots - 1):
        unit_load(n).start()
    gain_rows = jnp.transpose(gains[...])
    for q in range(rows // 128):
        gain_col[q * 128 : (q + 1) * 128, :] = jnp.broadcast_to(gain_rows[:, q : q + 1], (128, 128))
    pack()
    pl.semaphore_wait(barrier, count - 1 + groups - 1 + tps - 1)
    elsewhere(lambda j: dispatching(j).start())
    for n in range(len(sends)):
        do_unit(n)
        send_unit(*units[n][:2])

    land_x[t, z] = send_x[z]
    for other in range(1, tps):
        spreading(z, other).start()

    def forward(s):
        dispatched(s).wait_recv()
        for other in range(1, tps):
            spreading(s, other).start()

    elsewhere(forward)
    for n in range(len(sends), len(units)):
        do_unit(n)
    spread().wait_recv()
    normalise()
    gate_up(z, True)

    def take_piece(way, m, item, i, ready, wide=None):
        k = real(way, z)
        l, at = cut(i)

        mine = True if wide is None else (2 * k >= count) == wide

        @pl.when((item < k * (count - k)) & mine)
        def _():
            s = k - 1 - item // (count - k)
            dd = count - 1 - lax.rem(item, count - k)
            source = real(way, s)

            def awaited(ref):
                remote(
                    ref, ref, send_sem.at[0], recv_sem.at[way, item, m, i], "fs", source
                ).wait_recv()

            @pl.when(dd == k)
            def _():
                awaited(spot(m, l, at, source, y))
                ready(source, m, i)

            @pl.when(dd > k)
            def _():
                slot = (k - 1 - s) * (count - 1 - k) + (count - 1 - dd)
                ref = transit.at[way, slot, m, l, pl.ds(at, piece), :]
                awaited(ref)
                start_hop(way, ref, relay_sem.at[way, slot], m, i, k, s, dd)

    def settled(way, item, body, wide=None):
        k = real(way, z)
        kept = jnp.maximum(item, 0)
        s = k - 1 - kept // (count - k)
        dd = count - 1 - lax.rem(kept, count - k)

        mine = True if wide is None else (2 * k >= count) == wide

        @pl.when((item >= 0) & (item < k * (count - k)) & (dd == k) & mine)
        def _():
            body(real(way, s))

    def pass_on(source, m, i):
        for other in range(1, groups):
            passing(source, m, i, other).start()

    def await_pass(s, m, i):
        for other in range(1, groups):
            arriving(s, m, i, other).wait_recv()

    def early_block(s):
        def one(i, _):
            for m in (0, 1):
                await_pass(s, m, i)
            return 0

        lax.fori_loop(0, pieces, one, 0)
        gate_up(s, False)

    def early(n, _):
        for m in (0, 1):
            def one(i, _):
                for way in (0, 1):
                    take_piece(way, m, n, i, pass_on)
                return 0

            lax.fori_loop(0, pieces, one, 0)
            if m == 0:
                for way in (0, 1):
                    settled(way, n - 1, early_block)

        @pl.when(n == min(1, most - 1))
        def _():
            for r in range(count - 1):
                send_unit(r, 2)
        return 0

    lax.fori_loop(0, most + 1, early, 0)
    activate()
    def at_middle(body):
        @pl.when((z * (count - z) == most) | ((count - 1 - z) * (z + 1) == most))
        def _():
            for other in range(1, groups):
                body(other)

    at_middle(lambda other: lending(other).start())

    def own_down(i, _):
        down_piece(z, i, range(groups))
        return 0

    lax.fori_loop(0, pieces, own_down, 0)

    def sent(ref, sem):
        remote(ref, ref, sem, recv_sem.at[0, 0, 0, 0], "grp", lax.rem(y + 1, groups)).wait_send()

    def drain():
        for r in range(count - 1):
            sent(stage.at[r], send_sem.at[r])
            for m in range(3):
                base = pl.multiple_of(ranked(r) * rows + y * share, share)
                for other in range(1, groups):
                    sent(
                        landing[m].at[:, pl.ds(base, share), :],
                        pass_send.at[ranked(r), m, other - 1],
                    )
        for slot in range(transit.shape[1]):
            @pl.when(slot < z * (count - 1 - z))
            def _():
                for way in (0, 1):
                    sent(transit.at[way, slot], relay_sem.at[way, slot])

    def own_close(i, _):
        close_piece(i)
        return 0

    def whole(p):
        return p // pieces, lax.rem(p, pieces)

    def work(s, i):
        await_pass(s, 2, i)
        down_piece(s, i, range(groups))

    def later(wide, span):
        def one(p, _):
            n, i = whole(p)

            @pl.when(p < span)
            def _():
                for way in (0, 1):
                    take_piece(way, 2, n, i, pass_on, wide)

            def trail(lag, body):
                n, i = whole(jnp.maximum(p - lag, 0))
                due = (p >= lag) & (p < span + lag)
                for way in (0, 1):
                    settled(way, jnp.where(due, n, -1), lambda s: body(s, i), wide)

            def close(s, i):
                @pl.when(s == t)
                def _():
                    close_piece(i)

            trail(1, work)
            trail(3, close)
            return 0

        lax.fori_loop(0, span + 3, one, 0)

    def ending(i, _):
        for way in (0, 1):
            take_piece(way, 2, most - 1, i, pass_on)
        for way in (0, 1):
            settled(way, jnp.where(i >= 1, most - 1, -1), lambda s: work(s, jnp.maximum(i - 1, 0)))
        return 0

    narrow = max([k * (count - k) for k in range(count) if 2 * k < count])
    later(False, narrow * pieces)
    at_middle(lambda other: lent(other).wait_recv())

    @pl.when(z == t)
    def _():
        lax.fori_loop(0, pieces, own_close, 0)

    later(True, (most - 1) * pieces)
    lax.fori_loop(0, final, ending, 0)
    for way in (0, 1):
        def use(source, m, i, way=way):
            down_last(way, source)
            pass_on(source, m, i)

        take_piece(way, 2, most - 1, final, use)
    for way in (0, 1):
        settled(way, most - 1, lambda s: work(s, final - 1))

    inner = jnp.where(z < half, z + 1 < half, z - 1 >= half)
    outer = jnp.where(z < half, z - 1, z + 1)

    @pl.when(inner)
    def _():
        pl.semaphore_wait(go_sem, 1)

    @pl.when((outer >= 0) & (outer < count))
    def _():
        pl.semaphore_signal(go_sem, inc=1, device_id={"fs": outer}, device_id_type=MESH)

    @pl.when(last)
    def _():
        lax.fori_loop(0, pieces, own_close, 0)

    give_back()
    drain()

    def drain_more(i, _):
        for s in range(count):
            for giver in range(groups):
                skipped = comes_last(s) & (y != giver) & (i == final)

                @pl.when((s != t) & jnp.logical_not(skipped))
                def _():
                    part_copy(s, i, giver).wait_send()
        for way in (0, 1):
            k = real(way, z)

            @pl.when((k * (count - k) == most) & (i == final))
            def _():
                await_pass(real(way, 0), 2, i)
                for other in range(1, groups):
                    part_across(way, real(way, 0), other).wait_send()
        return 0

    lax.fori_loop(0, pieces, drain_more, 0)
    at_middle(lambda other: lending(other).wait_send())
    elsewhere(lambda j: dispatching(j).wait_send())
    spread().wait_send()

    elsewhere(lambda s: returned(s).wait_recv())
    back = land_ret[...].reshape(experts * capacity, columns)
    used = experts * capacity
    value = jnp.dot(combine_w[0, :, :used], back, preferred_element_type=f32)
    value = value + jnp.dot(combine_w[1, :, :used], back, preferred_element_type=f32)
    mixed_o[...] = value.astype(bf16)
    elsewhere(lambda j: returning(j).wait_send())


def writer_kernel(parts, *refs):
    ins, outs, sem = refs[:4], refs[4:8], refs[8]
    local, high = ins[0].shape[:2]
    step = high // parts

    def copy(k, l, i):
        at = pl.ds(i * step, step)
        return pltpu.make_async_copy(ins[k].at[l, at, :], outs[k].at[l, at, :], sem.at[k, l, i])

    small = pltpu.make_async_copy(ins[3], outs[3], sem.at[3, 0, 0])
    jobs = [copy(k, l, i) for k in range(3) for l in range(local) for i in range(parts)] + [small]
    for job in jobs:
        job.start()
    for job in jobs:
        job.wait()


def fused(tokens, routes, route_weights, norm_gain, gate_weight, up_weight, down_weight):
    groups, count, tps = (lax.axis_size(axis) for axis in ("grp", "fs", "tp"))
    experts, rows, width = gate_weight.shape
    local, own_tokens, columns = experts // count, *tokens.shape
    capacity = own_tokens * 5 // 16
    share = rows // groups
    parts = share // 128
    pieces = local * parts
    tall = count * capacity
    dims = (groups, count, tps, local, rows, width, parts, experts, capacity)
    shape = (local, count * rows, width)
    slots = max(1, max(k * (count - 1 - k) for k in range(count)))
    items = max(k * (count - k) for k in range(count))
    bf16, f32, sem = jnp.bfloat16, jnp.float32, pltpu.SemaphoreType.DMA
    vmem, anywhere = pl.BlockSpec(memory_space=pltpu.VMEM), pl.BlockSpec(memory_space=pl.ANY)
    block = (local * capacity, columns)
    gate, up, down, mixed, _ = pl.pallas_call(
        functools.partial(fused_kernel, dims),
        out_shape=[pltpu.VMEM(shape, bf16)] * 3
        + [pltpu.VMEM(tokens.shape, bf16)]
        + [jax.ShapeDtypeStruct((2, slots, 3, local, share, width), bf16)],
        in_specs=[vmem] * 4 + [anywhere] * 3,
        out_specs=[vmem] * 4 + [anywhere],
        scratch_shapes=[
            pltpu.VMEM((3, local, share, width), f32),
            pltpu.VMEM((count - 1, 3, local, share, width), bf16),
            pltpu.VMEM((rows, 128), f32),
            pltpu.VMEM((experts * capacity, 128), f32),
            pltpu.VMEM((count,) + block, bf16),
            pltpu.VMEM((tps, count) + block, bf16),
            pltpu.VMEM((local, tall, tps * columns), bf16),
            pltpu.VMEM((2, local, tall, width), f32),
            pltpu.VMEM((groups, local, tall, width), bf16),
            pltpu.VMEM((count, local, tall, columns), bf16),
            pltpu.VMEM((2, groups - 1, tall, 128), bf16),
            pltpu.VMEM((tps, local, tall, columns), bf16),
            pltpu.VMEM((2, own_tokens, -(-experts * capacity // 128) * 128), bf16),
            pltpu.VMEM((count,) + block, bf16),
            pltpu.VMEM((count,) + block, bf16),
            sem((3,)), sem((count - 1,)), sem((2, items, 3, pieces)), sem((2, slots)),
            sem((count, 3, groups - 1)), sem((count, 3, pieces, groups - 1)),
            sem((count,)), sem((count,)), sem((1,)), sem((1,)),
            sem((count, pieces, groups)), sem((tps, pieces, groups)), sem((count,)), sem((count,)),
            sem((2, groups - 1)), sem((groups,)), sem((groups,)),
            pltpu.SemaphoreType.REGULAR,
        ],
        compiler_params=pltpu.CompilerParams(
            collective_id=1, has_side_effects=True, vmem_limit_bytes=38 * 1024 * 1024
        ),
    )(
        tokens, routes.T, route_weights.T, norm_gain.reshape(rows // 128, 128),
        gate_weight, up_weight, down_weight,
    )
    parts = max(1, shape[1] // 512)
    return pl.pallas_call(
        functools.partial(writer_kernel, parts),
        out_shape=[jax.ShapeDtypeStruct(shape, bf16)] * 3
        + [jax.ShapeDtypeStruct(tokens.shape, bf16)],
        in_specs=[vmem] * 4,
        out_specs=[anywhere] * 4,
        scratch_shapes=[sem((4, local, parts))],
        compiler_params=pltpu.CompilerParams(vmem_limit_bytes=1024 * 1024),
    )(gate, up, down, mixed)


def on_device(tokens, routes, route_weights, norm_gain, gate_weight, up_weight, down_weight):
    groups, count, tps = (lax.axis_size(axis) for axis in ("grp", "fs", "tp"))
    experts, rows, width = gate_weight.shape
    own_tokens, columns = tokens.shape
    capacity = own_tokens * 5 // 16
    fits = (
        groups > 1 and 1 < count <= 8 and experts % count == 0 and rows == columns
        and count == tps and rows % (128 * groups) == 0 and width % 128 == 0
        and capacity % 8 == 0 and (experts // count * capacity) % 16 == 0
        and 6 * experts // count * count * rows * width <= 24 * 1024 * 1024
    )
    body = fused if fits else layered
    return tuple(
        body(tokens, routes, route_weights, norm_gain, gate_weight, up_weight, down_weight)
    )


def solution(mesh):
    in_specs = (
        P(("grp", "fs"), "tp"),
        P(("grp", "fs"), None),
        P(("grp", "fs"), None),
        P("fs"),
        P(None, "fs", "tp"),
        P(None, "fs", "tp"),
        P(None, "fs", "tp"),
    )
    out_specs = (
        P("fs", "grp", "tp"),
        P("fs", "grp", "tp"),
        P("fs", "grp", "tp"),
        P(("grp", "fs"), "tp"),
    )
    return jax.shard_map(
        on_device, mesh=mesh, in_specs=in_specs, out_specs=out_specs, check_vma=False
    )
```

```python
import functools

import jax
import jax.numpy as jnp
from jax import lax
from jax.experimental import pallas as pl
from jax.experimental.pallas import tpu as pltpu
from jax.sharding import PartitionSpec as P

epsilon = 1e-06
MESH = pl.DeviceIdType.MESH


def expert_slots(routes, experts, capacity):
    row_count = routes.shape[0] * routes.shape[1]
    flat_routes = routes.reshape(row_count)
    onehot = (flat_routes[:, None] == jnp.arange(experts, dtype=jnp.int32)[None, :]).astype(
        jnp.int32
    )
    earlier = jnp.cumsum(onehot, axis=0) - onehot
    position = jnp.sum(earlier * onehot, axis=1)
    return (flat_routes * capacity + position).reshape(routes.shape)


def dispatch(normed, slots, experts, capacity, copies, local_count):
    col_width = normed.shape[1]
    slot_ids = jnp.arange(experts * capacity, dtype=jnp.int32)
    select = jnp.any(slot_ids[:, None, None] == slots[None, :, :], axis=2).astype(jnp.bfloat16)
    packed = jnp.dot(select, normed, preferred_element_type=jnp.float32).astype(jnp.bfloat16)
    packed = jnp.broadcast_to(
        packed.reshape(experts, 1, capacity, col_width), (experts, copies, capacity, col_width)
    )
    return packed.reshape(experts * copies // local_count, local_count, capacity, col_width)


def combine(returned, slots, route_weights, experts, copies):
    capacity, col_width = (returned.shape[2], returned.shape[3])
    summed_up = jnp.sum(
        returned.reshape(experts, copies, capacity, col_width), axis=1, dtype=jnp.float32
    )
    selected = summed_up.reshape(experts * capacity, col_width)[slots]
    return jnp.sum(route_weights[:, :, None] * selected, axis=1)


def exchange_kernel(
    dims, gains, gate_w, up_w, down_w, gate_o, up_o, down_o,
    raw, stage, load_sem, send_sem, recv_sem, pass_send, pass_recv,
):
    groups, count, local, copies, rows, width, parts = dims
    weights, landing = (gate_w, up_w, down_w), (gate_o, up_o, down_o)
    y, z = lax.axis_index("grp"), lax.axis_index("fs")
    share = rows // groups
    piece = share // parts

    barrier = pltpu.get_barrier_semaphore()

    def greet(j, _):
        @pl.when(j != z)
        def _():
            pl.semaphore_signal(barrier, inc=1, device_id={"fs": j}, device_id_type=MESH)
        return 0

    lax.fori_loop(0, count, greet, 0)
    for other in range(1, groups):
        pl.semaphore_signal(
            barrier, inc=1, device_id={"grp": lax.rem(y + other, groups)}, device_id_type=MESH
        )

    def load(m, j, first, slot):
        if copies > 1:
            expert, column = j // copies, lax.rem(j, copies) * width
            column = pl.ds(pl.multiple_of(column, 128), width)
        else:
            expert, column = j * local, slice(None)
        return pltpu.make_async_copy(
            weights[m].at[pl.ds(expert, local), pl.ds(first, share), column],
            raw.at[slot], load_sem.at[slot],
        )

    def fold(m, slot, first, put):
        def one(i, _):
            l, q = i // parts, lax.rem(i, parts)
            at = pl.multiple_of(q * piece, piece)
            scaled = raw[slot, l, pl.ds(at, piece), :]
            if m < 2:
                scaled = scaled * gains[pl.ds(pl.multiple_of(first + at, piece), piece), :1]
            put(l, at, scaled.astype(jnp.bfloat16))
            return 0

        lax.fori_loop(0, local * parts, one, 0)

    def sending(j, m, i):
        l, q = i // parts, lax.rem(i, parts)
        at = pl.multiple_of(q * piece, piece)
        base = pl.multiple_of(z * rows + y * share + at, piece)
        return pltpu.make_async_remote_copy(
            src_ref=stage.at[j, m, l, pl.ds(at, piece), :],
            dst_ref=landing[m].at[l, pl.ds(base, piece), :],
            send_sem=send_sem.at[j, m, i],
            recv_sem=recv_sem.at[z, m, i],
            device_id={"fs": j}, device_id_type=MESH,
        )

    def passing(s, m, i, other):
        l, q = i // parts, lax.rem(i, parts)
        base = pl.multiple_of(s * rows + y * share + q * piece, piece)
        spot = landing[m].at[l, pl.ds(base, piece), :]
        return pltpu.make_async_remote_copy(
            src_ref=spot, dst_ref=spot,
            send_sem=pass_send.at[s, m, i, other - 1],
            recv_sem=pass_recv.at[s, m, i, other - 1],
            device_id={"grp": lax.rem(y + other, groups)}, device_id_type=MESH,
        )

    def arriving(s, m, i, other):
        l, q = i // parts, lax.rem(i, parts)
        giver = lax.rem(y + groups - other, groups)
        base = pl.multiple_of(s * rows + giver * share + q * piece, piece)
        spot = landing[m].at[l, pl.ds(base, piece), :]
        return pltpu.make_async_remote_copy(
            src_ref=spot, dst_ref=spot,
            send_sem=pass_send.at[s, m, i, other - 1],
            recv_sem=pass_recv.at[s, m, i, other - 1],
            device_id={"grp": giver}, device_id_type=MESH,
        )

    def landed(s, m, i):
        l, q = i // parts, lax.rem(i, parts)
        base = pl.multiple_of(s * rows + y * share + q * piece, piece)
        return pltpu.make_async_remote_copy(
            src_ref=landing[m].at[l, pl.ds(base, piece), :],
            dst_ref=landing[m].at[l, pl.ds(base, piece), :],
            send_sem=send_sem.at[s, m, i],
            recv_sem=recv_sem.at[s, m, i],
            device_id={"fs": s}, device_id_type=MESH,
        )

    mine = pl.multiple_of(y * share, share)
    pieces = local * parts

    def neighbours(body):
        def step(d, _):
            for j, there in ((z + d, z + d < count), (z - d, z - d >= 0)):
                @pl.when(there)
                def _():
                    body(j)
            return 0

        lax.fori_loop(1, count, step, 0)

    def send_phase(phase):
        def to(j):
            for m in phase:
                load(m, j, mine, m % 2).start()
            for m in phase:
                load(m, j, mine, m % 2).wait()

                def put(l, at, value):
                    stage[j, m, l, pl.ds(at, piece), :] = value

                fold(m, m % 2, mine, put)
            for m in phase:
                def go(i, _):
                    sending(j, m, i).start()
                    return 0

                lax.fori_loop(0, pieces, go, 0)

        neighbours(to)

    pl.semaphore_wait(barrier, count - 1 + groups - 1)
    send_phase((0, 1))
    send_phase((2,))

    for m in range(3):
        for g in range(groups):
            load(m, z, g * share, g % 2).start()
            load(m, z, g * share, g % 2).wait()

            def put(l, at, value):
                base = pl.multiple_of(z * rows + g * share + at, piece)
                landing[m][l, pl.ds(base, piece), :] = value

            fold(m, g % 2, g * share, put)

    def pass_phase(phase):
        def take(s):
            for m in phase:
                def one(i, _):
                    landed(s, m, i).wait_recv()
                    for other in range(1, groups):
                        passing(s, m, i, other).start()
                    return 0

                lax.fori_loop(0, pieces, one, 0)

        neighbours(take)

    pass_phase((0, 1))
    pass_phase((2,))

    def finish(s):
        for m in range(3):
            def one(i, _):
                for other in range(1, groups):
                    arriving(s, m, i, other).wait_recv()
                    passing(s, m, i, other).wait_send()
                sending(s, m, i).wait_send()
                return 0

            lax.fori_loop(0, pieces, one, 0)

    neighbours(finish)


def relay_kernel(
    dims, gains, gate_w, up_w, down_w, gate_o, up_o, down_o,
    raw, stage, transit, load_sem, send_sem, recv_sem, relay_sem, pass_send, pass_recv,
):
    groups, count, local, copies, rows, width, parts = dims
    weights, landing = (gate_w, up_w, down_w), (gate_o, up_o, down_o)
    y, z = lax.axis_index("grp"), lax.axis_index("fs")
    share = rows // groups
    piece = share // parts
    pieces = local * parts
    mine = pl.multiple_of(y * share, share)

    def real(way, place):
        return place if way == 0 else count - 1 - place

    barrier = pltpu.get_barrier_semaphore()
    for j, there in ((z + 1, z + 1 < count), (z - 1, z >= 1)):
        @pl.when(there)
        def _():
            pl.semaphore_signal(barrier, inc=1, device_id={"fs": j}, device_id_type=MESH)
    for other in range(1, groups):
        pl.semaphore_signal(
            barrier, inc=1, device_id={"grp": lax.rem(y + other, groups)}, device_id_type=MESH
        )

    def load(m, j, first, slot):
        if copies > 1:
            expert, column = j // copies, lax.rem(j, copies) * width
            column = pl.ds(pl.multiple_of(column, 128), width)
        else:
            expert, column = j * local, slice(None)
        return pltpu.make_async_copy(
            weights[m].at[pl.ds(expert, local), pl.ds(first, share), column],
            raw.at[slot], load_sem.at[slot],
        )

    def cut(i):
        return i // parts, pl.multiple_of(lax.rem(i, parts) * piece, piece)

    def fold(m, slot, first, put):
        def one(i, _):
            l, at = cut(i)
            scaled = raw[slot, l, pl.ds(at, piece), :]
            if m < 2:
                scaled = scaled * gains[pl.ds(pl.multiple_of(first + at, piece), piece), :1]
            put(l, at, scaled.astype(jnp.bfloat16))
            return 0

        lax.fori_loop(0, pieces, one, 0)

    def spot(m, l, at, source, giver):
        base = pl.multiple_of(source * rows + giver * share + at, piece)
        return landing[m].at[l, pl.ds(base, piece), :]

    def hop(way, src, sem, m, i, k, s, dd, final):
        l, at = cut(i)
        if final:
            dst = spot(m, l, at, real(way, s), y)
        else:
            slot = (k - s) * (count - 2 - k) + (count - 1 - dd)
            dst = transit.at[way, slot, m, l, pl.ds(at, piece), :]
        place = (k - s) * (count - 1 - k) + (count - 1 - dd)
        return pltpu.make_async_remote_copy(
            src_ref=src, dst_ref=dst, send_sem=sem,
            recv_sem=recv_sem.at[way, place, m, i],
            device_id={"fs": real(way, k + 1)}, device_id_type=MESH,
        )

    def start_hop(way, src, sem, m, i, k, s, dd):
        @pl.when(dd == k + 1)
        def _():
            hop(way, src, sem, m, i, k, s, dd, True).start()

        @pl.when(dd > k + 1)
        def _():
            hop(way, src, sem, m, i, k, s, dd, False).start()

    def passing(s, m, i, other):
        l, at = cut(i)
        ref = spot(m, l, at, s, y)
        return pltpu.make_async_remote_copy(
            src_ref=ref, dst_ref=ref,
            send_sem=pass_send.at[s, m, i, other - 1],
            recv_sem=pass_recv.at[s, m, i, other - 1],
            device_id={"grp": lax.rem(y + other, groups)}, device_id_type=MESH,
        )

    def arriving(s, m, i, other):
        l, at = cut(i)
        giver = lax.rem(y + groups - other, groups)
        ref = spot(m, l, at, s, giver)
        return pltpu.make_async_remote_copy(
            src_ref=ref, dst_ref=ref,
            send_sem=pass_send.at[s, m, i, other - 1],
            recv_sem=pass_recv.at[s, m, i, other - 1],
            device_id={"grp": giver}, device_id_type=MESH,
        )

    def send_phase(phase):
        def step(d, _):
            for way in (0, 1):
                k = real(way, z)
                dd = count - d
                j = real(way, dd)

                @pl.when(dd > k)
                def _():
                    for m in phase:
                        load(m, j, mine, m).start()
                    for m in phase:
                        load(m, j, mine, m).wait()

                        def put(l, at, value):
                            stage[j, m, l, pl.ds(at, piece), :] = value

                        fold(m, m, mine, put)

                        def go(i, _):
                            l, at = cut(i)
                            src = stage.at[j, m, l, pl.ds(at, piece), :]
                            start_hop(way, src, send_sem.at[j, m, i], m, i, k, k, dd)
                            return 0

                        lax.fori_loop(0, pieces, go, 0)
            return 0

        lax.fori_loop(1, count, step, 0)

    def own_block():
        for m in range(3):
            for g in range(groups):
                load(m, z, g * share, g % 2).start()
                load(m, z, g * share, g % 2).wait()

                def put(l, at, value):
                    stage[z, m, l, pl.ds(at, piece), :] = value

                fold(m, g % 2, g * share, put)
                base = pl.multiple_of(z * rows + g * share, share)
                keep = pltpu.make_async_copy(
                    stage.at[z, m], landing[m].at[:, pl.ds(base, share), :], load_sem.at[g % 2]
                )
                keep.start()
                keep.wait()

    def take_phase(phase):
        most = max(k * (count - k) for k in range(count))

        def take(item, _):
            for m in phase:
                def one(i, _):
                    l, at = cut(i)
                    for way in (0, 1):
                        take_piece(way, m, item, i, l, at)
                    return 0

                lax.fori_loop(0, pieces, one, 0)
            return 0

        lax.fori_loop(0, most, take, 0)

    def take_piece(way, m, item, i, l, at):
        k = real(way, z)

        @pl.when(item < k * (count - k))
        def _():
            s = k - 1 - item // (count - k)
            dd = count - 1 - lax.rem(item, count - k)
            source = real(way, s)

            def awaited(ref):
                pltpu.make_async_remote_copy(
                    src_ref=ref, dst_ref=ref, send_sem=send_sem.at[source, m, i],
                    recv_sem=recv_sem.at[way, item, m, i],
                    device_id={"fs": source}, device_id_type=MESH,
                ).wait_recv()

            @pl.when(dd == k)
            def _():
                awaited(spot(m, l, at, source, y))
                for other in range(1, groups):
                    passing(source, m, i, other).start()

            @pl.when(dd > k)
            def _():
                slot = (k - 1 - s) * (count - 1 - k) + (count - 1 - dd)
                ref = transit.at[way, slot, m, l, pl.ds(at, piece), :]
                awaited(ref)
                start_hop(way, ref, relay_sem.at[way, slot, m, i], m, i, k, s, dd)

    def sent(ref, sem):
        pltpu.make_async_remote_copy(
            src_ref=ref, dst_ref=ref, send_sem=sem, recv_sem=recv_sem.at[0, 0, 0, 0],
            device_id={"grp": lax.rem(y + 1, groups)}, device_id_type=MESH,
        ).wait_send()

    def finish():
        def block(t, _):
            s, i = t // pieces, lax.rem(t, pieces)
            l, at = cut(i)

            @pl.when(s != z)
            def _():
                for m in range(3):
                    for other in range(1, groups):
                        arriving(s, m, i, other).wait_recv()
                        passing(s, m, i, other).wait_send()
                    sent(stage.at[s, m, l, pl.ds(at, piece), :], send_sem.at[s, m, i])
            return 0

        lax.fori_loop(0, count * pieces, block, 0)

        def passed(t, _):
            slot, i = t // pieces, lax.rem(t, pieces)
            l, at = cut(i)
            for way in (0, 1):
                @pl.when(slot < z * (count - 1 - z))
                def _():
                    for m in range(3):
                        sent(
                            transit.at[way, slot, m, l, pl.ds(at, piece), :],
                            relay_sem.at[way, slot, m, i],
                        )
            return 0

        lax.fori_loop(0, transit.shape[1] * pieces, passed, 0)

    ends = (z == 0).astype(jnp.int32) + (z == count - 1).astype(jnp.int32)
    pl.semaphore_wait(barrier, 2 - ends + groups - 1)
    send_phase((0, 1, 2))
    own_block()
    take_phase((0, 1, 2))
    finish()


def exchange(norm_gain, gate_weight, up_weight, down_weight, groups, count, copies, local):
    experts, rows, columns = gate_weight.shape
    width = columns // copies
    share = rows // groups
    parts = max(1, share // 128)
    gains = jnp.broadcast_to(norm_gain[:, None], (rows, 128))
    shape = (local, count * rows, width)
    dims = (groups, count, local, copies, rows, width, parts)
    pieces = local * parts
    relaying = 1 < count <= 8 and groups > 1
    common = [
        pltpu.VMEM((3, local, share, width), jnp.float32),
        pltpu.VMEM((count, 3, local, share, width), jnp.bfloat16),
    ]
    sem = pltpu.SemaphoreType.DMA
    passes = [sem((count, 3, pieces, max(1, groups - 1)))] * 2
    if relaying:
        slots = max(1, max(k * (count - 1 - k) for k in range(count)))
        items = max(k * (count - k) for k in range(count))
        scratch = common + [
            pltpu.VMEM((2, slots, 3, local, share, width), jnp.bfloat16),
            sem((3,)), sem((count, 3, pieces)), sem((2, items, 3, pieces)),
            sem((2, slots, 3, pieces)),
        ] + passes
    else:
        scratch = common + [sem((2,))] + [sem((count, 3, pieces))] * 2 + passes
    return pl.pallas_call(
        functools.partial(relay_kernel if relaying else exchange_kernel, dims),
        out_shape=[jax.ShapeDtypeStruct(shape, jnp.bfloat16)] * 3,
        in_specs=[pl.BlockSpec(memory_space=pltpu.VMEM)]
        + [pl.BlockSpec(memory_space=pl.ANY)] * 3,
        out_specs=[pl.BlockSpec(memory_space=pl.ANY if relaying else pltpu.VMEM)] * 3,
        scratch_shapes=scratch,
        compiler_params=pltpu.CompilerParams(
            collective_id=0, has_side_effects=True, vmem_limit_bytes=60 * 1024 * 1024
        ),
    )(gains, gate_weight, up_weight, down_weight)


def layered(tokens, routes, route_weights, norm_gain, gate_weight, up_weight, down_weight):
    groups = lax.axis_size("grp")
    fs_count = lax.axis_size("fs")
    tp_count = lax.axis_size("tp")
    experts = gate_weight.shape[0]
    copies = max(1, fs_count // experts)
    local_count = max(1, experts // fs_count)
    capacity = tokens.shape[0] * 5 // 16

    gate_new, up_new, down_new = exchange(
        norm_gain, gate_weight, up_weight, down_weight, groups, fs_count, copies, local_count
    )
    slots = expert_slots(routes, experts, capacity)
    whole = lax.all_gather(tokens, "tp", axis=1, tiled=True)
    widened = whole.astype(jnp.float32)
    row_scale = lax.rsqrt(jnp.mean(widened * widened, axis=1, keepdims=True) + epsilon)
    normed = (widened * row_scale).astype(jnp.bfloat16)
    outgoing = dispatch(normed, slots, experts, capacity, copies, local_count)
    arrived = lax.all_to_all(outgoing, "fs", split_axis=0, concat_axis=0, tiled=True)
    gate_sums = jnp.einsum("slcd,ldf->slcf", arrived, gate_new, preferred_element_type=jnp.float32)
    up_sums = jnp.einsum("slcd,ldf->slcf", arrived, up_new, preferred_element_type=jnp.float32)
    hidden = (jax.nn.silu(gate_sums) * up_sums).astype(jnp.bfloat16)
    partial_value = jnp.einsum(
        "slcf,ldf->slcd", hidden, down_new, preferred_element_type=jnp.float32
    ).astype(jnp.bfloat16)
    by_columns = partial_value.reshape(
        partial_value.shape[:3] + (tp_count, partial_value.shape[3] // tp_count)
    )
    exchanged = lax.all_to_all(by_columns, "tp", split_axis=3, concat_axis=3, tiled=True)
    summed_up = jnp.sum(exchanged, axis=3, dtype=jnp.float32)
    handed = lax.all_to_all(
        summed_up.astype(jnp.bfloat16), "fs", split_axis=0, concat_axis=0, tiled=True
    ).astype(summed_up.dtype)
    combined = combine(handed, slots, route_weights, experts, copies)
    return (gate_new, up_new, down_new, combined.astype(jnp.bfloat16))


def far_first(count):
    table = []
    for z in range(count):
        right = [j for j in range(count - 1, z, -1)]
        left = [j for j in range(z)]
        ways, order = sorted((right, left), key=len, reverse=True), []
        for d in range(count):
            order += [way[d] for way in ways if d < len(way)]
        table.append(order)
    return table


def mates(count):
    paired = count & (count - 1) == 0
    return [[k ^ d if paired else (k + d) % count for k in range(count)] for d in range(count)]


def fused_kernel(dims, *refs):
    count = dims[1]
    (tokens, routes, route_weights, gains, gate_w, up_w, down_w), refs = refs[:7], refs[7:]
    (gate_o, up_o, down_o, transit, combine_w), refs = refs[:5], refs[5:]
    back_o, refs = refs[:count], refs[count:]
    (
        raw, stage, gain_col, scales, send_x, land_x, normed, sums, hidden, partial, across, summing,
        load_sem, send_sem, recv_sem, relay_sem, pass_send, pass_recv,
        x_send, x_recv, xg_send, xg_recv, part_send, part_recv, across_send, hid_send, hid_recv,
    ) = refs
    groups, count, tps, local, rows, width, parts, experts, capacity = dims
    weights, landing = (gate_w, up_w, down_w), (gate_o, up_o, down_o)
    y, z, t = lax.axis_index("grp"), lax.axis_index("fs"), lax.axis_index("tp")
    share = rows // groups
    piece = share // parts
    pieces = local * parts
    mine = pl.multiple_of(y * share, share)
    table = far_first(count)
    block_rows = local * capacity
    own_tokens, columns = tokens.shape
    tall = count * capacity
    f32, bf16 = jnp.float32, jnp.bfloat16

    def ranked(r):
        return sum((z == k).astype(jnp.int32) * table[k][r] for k in range(count))

    def real(way, place):
        return place if way == 0 else count - 1 - place

    def remote(src, dst, send, recv, axis, index):
        return pltpu.make_async_remote_copy(
            src_ref=src, dst_ref=dst, send_sem=send, recv_sem=recv,
            device_id={axis: index}, device_id_type=MESH,
        )

    barrier = pltpu.get_barrier_semaphore()
    for axis, me, size in (("fs", z, count), ("grp", y, groups), ("tp", t, tps)):
        for other in range(1, size):
            pl.semaphore_signal(
                barrier, inc=1, device_id={axis: lax.rem(me + other, size)}, device_id_type=MESH
            )

    def load(m, j, first, slot):
        return pltpu.make_async_copy(
            weights[m].at[pl.ds(j * local, local), pl.ds(first, share), :],
            raw.at[slot], load_sem.at[slot],
        )

    def cut(i):
        return i // parts, pl.multiple_of(lax.rem(i, parts) * piece, piece)

    def fold(m, slot, first, put):
        def one(i, _):
            l, at = cut(i)
            scaled = raw[slot, l, pl.ds(at, piece), :]
            if m < 2:
                scaled = scaled * gain_col[pl.ds(pl.multiple_of(first + at, piece), piece), :1]
            put(l, at, scaled.astype(bf16))
            return 0

        lax.fori_loop(0, pieces, one, 0)

    def spot(m, l, at, source, giver):
        base = pl.multiple_of(source * rows + giver * share + at, piece)
        return landing[m].at[l, pl.ds(base, piece), :]

    def start_hop(way, src, sem, m, i, k, s, dd):
        l, at = cut(i)
        place = (k - s) * (count - 1 - k) + (count - 1 - dd)
        recv = recv_sem.at[way, place, m, i]

        @pl.when(dd == k + 1)
        def _():
            remote(src, spot(m, l, at, real(way, s), y), sem, recv, "fs", real(way, k + 1)).start()

        @pl.when(dd > k + 1)
        def _():
            slot = (k - s) * (count - 2 - k) + (count - 1 - dd)
            dst = transit.at[way, slot, m, l, pl.ds(at, piece), :]
            remote(src, dst, sem, recv, "fs", real(way, k + 1)).start()

    def passing(s, m, i, other):
        l, at = cut(i)
        ref = spot(m, l, at, s, y)
        return remote(
            ref, ref, pass_send.at[s, m, other - 1], pass_recv.at[s, m, i, other - 1],
            "grp", lax.rem(y + other, groups),
        )

    def arriving(s, m, i, other):
        l, at = cut(i)
        giver = lax.rem(y + groups - other, groups)
        ref = spot(m, l, at, s, giver)
        return remote(
            ref, ref, pass_send.at[s, m, other - 1], pass_recv.at[s, m, i, other - 1],
            "grp", giver,
        )

    def slot_rows():
        wanted = routes[...]
        expert_ids = lax.broadcasted_iota(jnp.int32, (experts, own_tokens), 0)
        onehots = [
            (expert_ids == wanted[k : k + 1, :]).astype(f32) for k in range(wanted.shape[0])
        ]
        before = lax.broadcasted_iota(jnp.int32, (own_tokens, own_tokens), 0)
        after = lax.broadcasted_iota(jnp.int32, (own_tokens, own_tokens), 1)
        upper = (before < after).astype(bf16)
        earlier = jnp.dot(sum(onehots).astype(bf16), upper, preferred_element_type=f32)
        found = []
        for k, onehot in enumerate(onehots):
            position = jnp.sum(earlier * onehot, axis=0, keepdims=True)
            earlier = earlier + onehot
            found.append(wanted[k : k + 1, :] * capacity + position.astype(jnp.int32))
        return found

    def pack():
        found = slot_rows()
        shape = (experts * capacity, own_tokens)
        slot_ids = lax.broadcasted_iota(jnp.int32, shape, 0)
        chosen = jnp.zeros(shape, f32)
        for slot in found:
            chosen = jnp.where(slot_ids == slot, 1.0, chosen)
        packed = jnp.dot(chosen.astype(bf16), tokens[...], preferred_element_type=f32)
        packed = packed.astype(bf16)
        for j in range(count):
            send_x[j] = packed[j * block_rows : (j + 1) * block_rows, :]

    def weigh():
        found = slot_rows()
        shape = (combine_w.shape[3], own_tokens)
        places = lax.broadcasted_iota(jnp.int32, shape, 0)
        for d in range(count):
            source = sum(
                (z == k).astype(jnp.int32) * mates(count)[d].index(k) for k in range(count)
            )
            first = source * block_rows
            weighed = jnp.zeros(shape, f32)
            for k, slot in enumerate(found):
                hit = (places + first == slot) & (places < block_rows)
                weighed = weighed + jnp.where(hit, route_weights[k : k + 1, :], 0.0)
            weighed = jnp.transpose(weighed)
            high = weighed.astype(bf16)
            combine_w[d, 0] = high
            combine_w[d, 1] = (weighed - high.astype(f32)).astype(bf16)

    def dispatching(j):
        return remote(send_x.at[j], land_x.at[t, z], x_send.at[j], x_recv.at[z], "fs", j)

    def dispatched(s):
        return remote(send_x.at[s], land_x.at[t, s], x_send.at[s], x_recv.at[s], "fs", s)

    def spreading(s, other):
        return remote(
            land_x.at[t, s], land_x.at[t, s], xg_send.at[0], xg_recv.at[0],
            "tp", lax.rem(t + other, tps),
        )

    def spread():
        ref = land_x.at[pl.ds(0, tps - 1)]
        return remote(ref, ref, xg_send.at[0], xg_recv.at[0], "tp", lax.rem(t + 1, tps))

    def elsewhere(body):
        for other in range(1, count):
            body(lax.rem(z + other, count))

    def normalise():
        for s in range(count):
            square = jnp.zeros((block_rows, 1), f32)
            for c in range(tps):
                part = land_x[c, s].astype(f32)
                square = square + jnp.sum(part * part, axis=1, keepdims=True)
            scales[s * block_rows : (s + 1) * block_rows, :] = jnp.broadcast_to(
                lax.rsqrt(square / (tps * columns) + epsilon), (block_rows, 128)
            )
        for c in range(tps):
            pile = [[] for _ in range(local)]
            for s in range(count):
                scale = scales[s * block_rows : (s + 1) * block_rows, :1]
                scaled = land_x[c, s].astype(f32) * scale
                for l in range(local):
                    pile[l].append(scaled[l * capacity : (l + 1) * capacity, :])
            for l in range(local):
                normed[l, :, c * columns : (c + 1) * columns] = jnp.concatenate(
                    pile[l], axis=0
                ).astype(bf16)

    tile = min(width, 256)

    def gate_up(s, first):
        def one(i, _):
            l, n = i // (width // tile), lax.rem(i, width // tile)
            base, at = pl.multiple_of(s * rows, rows), pl.multiple_of(n * tile, tile)
            x = normed[l, :, pl.ds(base, rows)]
            for m in range(2):
                w = landing[m][l, pl.ds(base, rows), pl.ds(at, tile)]
                value = jnp.dot(x, w, preferred_element_type=f32)
                if not first:
                    value = value + sums[m, l, :, pl.ds(at, tile)]
                sums[m, l, :, pl.ds(at, tile)] = value
            return 0

        lax.fori_loop(0, local * (width // tile), one, 0)

    def activate():
        def one(i, _):
            l, n = i // (width // tile), lax.rem(i, width // tile)
            at = pl.multiple_of(n * tile, tile)
            value = jax.nn.silu(sums[0, l, :, pl.ds(at, tile)]) * sums[1, l, :, pl.ds(at, tile)]
            hidden[y, l, :, pl.ds(at, tile)] = value.astype(bf16)
            return 0

        lax.fori_loop(0, local * (width // tile), one, 0)

    most = max(k * (count - k) for k in range(count))

    def comes_last(s):
        place = jnp.where(z > s, z, count - 1 - z)
        origin = jnp.where(z > s, s, count - 1 - s)
        arrival = (place - 1 - origin) * (count - place) + (count - 1 - place)
        return (z != s) & (arrival == most - 1)

    last = comes_last(t)

    def feature(giver, at):
        return pl.ds(pl.multiple_of(giver * share + at, piece), piece)

    def lending(other):
        return pltpu.make_async_remote_copy(
            src_ref=hidden.at[y, local - 1], dst_ref=hidden.at[y, local - 1],
            send_sem=hid_send.at[other], recv_sem=hid_recv.at[y], device_id={"grp": lax.rem(y + other, groups)},
            device_id_type=MESH,
        )

    def lent(other):
        giver = lax.rem(y + other, groups)
        ref = hidden.at[giver, local - 1]
        return remote(ref, ref, hid_send.at[other], hid_recv.at[giver], "grp", giver)

    def part_copy(s, i, giver):
        l, at = cut(i)
        col = feature(giver, at)
        return remote(
            partial.at[s, l, :, col], summing.at[t, l, :, col], part_send.at[s, i, giver],
            part_recv.at[t, i, giver], "tp", s,
        )

    final = pieces - 1

    def part_across(way, s, other):
        l, at = cut(final)
        return pltpu.make_async_remote_copy(
            src_ref=across.at[way, other - 1],
            dst_ref=summing.at[t, l, :, feature(y, at)],
            send_sem=across_send.at[way, other - 1], recv_sem=part_recv.at[t, final, y],
            device_id={"grp": lax.rem(y + other, groups), "tp": s}, device_id_type=MESH,
        )

    def part_here(peer, i, giver):
        l, at = cut(i)
        ref = summing.at[peer, l, :, feature(giver, at)]
        return remote(ref, ref, part_send.at[0, i, giver], part_recv.at[peer, i, giver], "tp", peer)

    def down_rows(group, s, i, giver):
        l, at = cut(i)
        base = pl.multiple_of(s * rows + giver * share + at, piece)
        return lax.dot_general(
            hidden[group, l], down_o[l, pl.ds(base, piece), :], (((1,), (1,)), ((), ())),
            preferred_element_type=f32,
        ).astype(bf16)

    def down_piece(s, i, givers):
        l, at = cut(i)
        for giver in givers:
            value = down_rows(y, s, i, giver)

            @pl.when(s == t)
            def _():
                summing[t, l, :, feature(giver, at)] = value

            @pl.when(s != t)
            def _():
                partial[s, l, :, feature(giver, at)] = value

        @pl.when(s != t)
        def _():
            for giver in givers:
                part_copy(s, i, giver).start()

    def down_last(way, s):
        for other in range(1, groups):
            across[way, other - 1] = down_rows(lax.rem(y + other, groups), s, final, y)
        down_piece(s, final, (y,))
        for other in range(1, groups):
            part_across(way, s, other).start()

    def close_piece(i):
        l, at = cut(i)
        for giver in range(groups):
            for other in range(1, tps):
                part_here(lax.rem(t + other, tps), i, giver).wait_recv()

            @pl.when((y != giver) & last & (i == final))
            def _():
                part_here(t, i, giver).wait_recv()

            col = feature(giver, at)
            value = summing[0, l, :, col].astype(f32)
            for peer in range(1, tps):
                value = value + summing[peer, l, :, col].astype(f32)
            sums[0, l, :, col] = value

    def give_back():
        for d in range(count):
            target = sum((z == k).astype(jnp.int32) * mates(count)[d][k] for k in range(count))
            first = pl.multiple_of(target * capacity, 8)
            back_o[d][...] = jnp.concatenate(
                [sums[0, l, pl.ds(first, capacity), :columns] for l in range(local)], axis=0
            ).astype(bf16)

    sends = [(r, m, None) for r in range(count - 1) for m in (0, 1)]
    keeps = [(None, m, g) for m in (0, 1) for g in range(groups)]
    late = [(r, 2, None) for r in range(count - 1)] + [(None, 2, g) for g in range(groups)]
    units = sends + keeps + late
    slots = raw.shape[0]

    def unit_load(n):
        r, m, g = units[n]
        if g is None:
            return load(m, ranked(r), mine, n % slots)
        return load(m, z, g * share, n % slots)

    def send_unit(r, m):
        j = ranked(r)

        def go(i, _):
            l, at = cut(i)
            src = stage.at[r, m, l, pl.ds(at, piece), :]
            for way in (0, 1):
                @pl.when(j > z if way == 0 else j < z)
                def _():
                    start_hop(
                        way, src, send_sem.at[r], m, i, real(way, z), real(way, z),
                        real(way, j),
                    )
            return 0

        lax.fori_loop(0, pieces, go, 0)

    def do_unit(n):
        r, m, g = units[n]
        if n + slots - 1 < len(units):
            unit_load(n + slots - 1).start()
        unit_load(n).wait()
        if g is None:
            def put(l, at, value):
                stage[r, m, l, pl.ds(at, piece), :] = value

            fold(m, n % slots, mine, put)
        else:
            def put(l, at, value):
                base = pl.multiple_of(z * rows + g * share + at, piece)
                landing[m][l, pl.ds(base, piece), :] = value

            fold(m, n % slots, g * share, put)

    for n in range(slots - 1):
        unit_load(n).start()
    gain_rows = jnp.transpose(gains[...])
    for q in range(rows // 128):
        gain_col[q * 128 : (q + 1) * 128, :] = jnp.broadcast_to(gain_rows[:, q : q + 1], (128, 128))
    pack()
    pl.semaphore_wait(barrier, count - 1 + groups - 1 + tps - 1)
    elsewhere(lambda j: dispatching(j).start())
    for n in range(len(sends)):
        do_unit(n)
        send_unit(*units[n][:2])

    land_x[t, z] = send_x[z]
    for other in range(1, tps):
        spreading(z, other).start()

    def forward(s):
        dispatched(s).wait_recv()
        for other in range(1, tps):
            spreading(s, other).start()

    elsewhere(forward)
    for n in range(len(sends), len(units)):
        do_unit(n)
    spread().wait_recv()
    weigh()
    normalise()
    gate_up(z, True)

    def take_piece(way, m, item, i, ready, wide=None):
        k = real(way, z)
        l, at = cut(i)

        mine = True if wide is None else (2 * k >= count) == wide

        @pl.when((item < k * (count - k)) & mine)
        def _():
            s = k - 1 - item // (count - k)
            dd = count - 1 - lax.rem(item, count - k)
            source = real(way, s)

            def awaited(ref):
                remote(
                    ref, ref, send_sem.at[0], recv_sem.at[way, item, m, i], "fs", source
                ).wait_recv()

            @pl.when(dd == k)
            def _():
                awaited(spot(m, l, at, source, y))
                ready(source, m, i)

            @pl.when(dd > k)
            def _():
                slot = (k - 1 - s) * (count - 1 - k) + (count - 1 - dd)
                ref = transit.at[way, slot, m, l, pl.ds(at, piece), :]
                awaited(ref)
                start_hop(way, ref, relay_sem.at[way, slot], m, i, k, s, dd)

    def settled(way, item, body, wide=None):
        k = real(way, z)
        kept = jnp.maximum(item, 0)
        s = k - 1 - kept // (count - k)
        dd = count - 1 - lax.rem(kept, count - k)

        mine = True if wide is None else (2 * k >= count) == wide

        @pl.when((item >= 0) & (item < k * (count - k)) & (dd == k) & mine)
        def _():
            body(real(way, s))

    def pass_on(source, m, i):
        for other in range(1, groups):
            passing(source, m, i, other).start()

    def await_pass(s, m, i):
        for other in range(1, groups):
            arriving(s, m, i, other).wait_recv()

    def early_block(s):
        def one(i, _):
            for m in (0, 1):
                await_pass(s, m, i)
            return 0

        lax.fori_loop(0, pieces, one, 0)
        gate_up(s, False)

    def early(n, _):
        for m in (0, 1):
            def one(i, _):
                for way in (0, 1):
                    take_piece(way, m, n, i, pass_on)
                return 0

            lax.fori_loop(0, pieces, one, 0)
            if m == 0:
                for way in (0, 1):
                    settled(way, n - 1, early_block)

        @pl.when(n == min(1, most - 1))
        def _():
            for r in range(count - 1):
                send_unit(r, 2)
        return 0

    lax.fori_loop(0, most + 1, early, 0)
    activate()
    def at_middle(body):
        @pl.when((z * (count - z) == most) | ((count - 1 - z) * (z + 1) == most))
        def _():
            for other in range(1, groups):
                body(other)

    at_middle(lambda other: lending(other).start())

    def own_down(i, _):
        down_piece(z, i, range(groups))
        return 0

    lax.fori_loop(0, pieces, own_down, 0)

    def sent(ref, sem):
        remote(ref, ref, sem, recv_sem.at[0, 0, 0, 0], "grp", lax.rem(y + 1, groups)).wait_send()

    def drain():
        for r in range(count - 1):
            sent(stage.at[r], send_sem.at[r])
            for m in range(3):
                base = pl.multiple_of(ranked(r) * rows + y * share, share)
                for other in range(1, groups):
                    sent(
                        landing[m].at[:, pl.ds(base, share), :],
                        pass_send.at[ranked(r), m, other - 1],
                    )
        for slot in range(transit.shape[1]):
            @pl.when(slot < z * (count - 1 - z))
            def _():
                for way in (0, 1):
                    sent(transit.at[way, slot], relay_sem.at[way, slot])

    def own_close(i, _):
        close_piece(i)
        return 0

    def whole(p):
        return p // pieces, lax.rem(p, pieces)

    def work(s, i):
        await_pass(s, 2, i)
        down_piece(s, i, range(groups))

    def later(wide, span):
        def one(p, _):
            n, i = whole(p)

            @pl.when(p < span)
            def _():
                for way in (0, 1):
                    take_piece(way, 2, n, i, pass_on, wide)

            def trail(lag, body):
                n, i = whole(jnp.maximum(p - lag, 0))
                due = (p >= lag) & (p < span + lag)
                for way in (0, 1):
                    settled(way, jnp.where(due, n, -1), lambda s: body(s, i), wide)

            def close(s, i):
                @pl.when(s == t)
                def _():
                    close_piece(i)

            trail(1, work)
            trail(3, close)
            return 0

        lax.fori_loop(0, span + 3, one, 0)

    def ending(i, _):
        for way in (0, 1):
            take_piece(way, 2, most - 1, i, pass_on)
        for way in (0, 1):
            settled(way, jnp.where(i >= 1, most - 1, -1), lambda s: work(s, jnp.maximum(i - 1, 0)))
        return 0

    narrow = max([k * (count - k) for k in range(count) if 2 * k < count])
    later(False, narrow * pieces)
    at_middle(lambda other: lent(other).wait_recv())

    @pl.when(z == t)
    def _():
        lax.fori_loop(0, pieces, own_close, 0)

    later(True, (most - 1) * pieces)
    lax.fori_loop(0, final, ending, 0)
    for way in (0, 1):
        def use(source, m, i, way=way):
            down_last(way, source)
            pass_on(source, m, i)

        take_piece(way, 2, most - 1, final, use)
    for way in (0, 1):
        settled(way, most - 1, lambda s: work(s, final - 1))

    @pl.when(last)
    def _():
        lax.fori_loop(0, pieces, own_close, 0)

    give_back()
    drain()

    def drain_more(i, _):
        for s in range(count):
            for giver in range(groups):
                skipped = comes_last(s) & (y != giver) & (i == final)

                @pl.when((s != t) & jnp.logical_not(skipped))
                def _():
                    part_copy(s, i, giver).wait_send()
        for way in (0, 1):
            k = real(way, z)

            @pl.when((k * (count - k) == most) & (i == final))
            def _():
                await_pass(real(way, 0), 2, i)
                for other in range(1, groups):
                    part_across(way, real(way, 0), other).wait_send()
        return 0

    lax.fori_loop(0, pieces, drain_more, 0)
    at_middle(lambda other: lending(other).wait_send())
    elsewhere(lambda j: dispatching(j).wait_send())
    spread().wait_send()


def writer_kernel(parts, *refs):
    ins, outs, sem = refs[:3], refs[3:6], refs[6]
    local, high = ins[0].shape[:2]
    step = high // parts

    def copy(k, l, i):
        at = pl.ds(i * step, step)
        return pltpu.make_async_copy(ins[k].at[l, at, :], outs[k].at[l, at, :], sem.at[k, l, i])

    jobs = [copy(k, l, i) for k in range(3) for l in range(local) for i in range(parts)]
    for job in jobs:
        job.start()
    for job in jobs:
        job.wait()


def combine_kernel(weights, *refs):
    value = None
    for d, back in enumerate(refs[:-1]):
        for part in range(2):
            term = jnp.dot(
                weights[d, part, :, : back.shape[0]], back[...],
                preferred_element_type=jnp.float32,
            )
            value = term if value is None else value + term
    refs[-1][...] = value.astype(refs[-1].dtype)


def fused(tokens, routes, route_weights, norm_gain, gate_weight, up_weight, down_weight):
    groups, count, tps = (lax.axis_size(axis) for axis in ("grp", "fs", "tp"))
    experts, rows, width = gate_weight.shape
    local, own_tokens, columns = experts // count, *tokens.shape
    capacity = own_tokens * 5 // 16
    share = rows // groups
    parts = share // 128
    pieces = local * parts
    tall = count * capacity
    dims = (groups, count, tps, local, rows, width, parts, experts, capacity)
    shape = (local, count * rows, width)
    slots = max(1, max(k * (count - 1 - k) for k in range(count)))
    items = max(k * (count - k) for k in range(count))
    bf16, f32, sem = jnp.bfloat16, jnp.float32, pltpu.SemaphoreType.DMA
    vmem, anywhere = pl.BlockSpec(memory_space=pltpu.VMEM), pl.BlockSpec(memory_space=pl.ANY)
    block = (local * capacity, columns)
    lanes = -(-block[0] // 128) * 128
    gate, up, down, _, weights, *backs = pl.pallas_call(
        functools.partial(fused_kernel, dims),
        out_shape=[pltpu.VMEM(shape, bf16)] * 3
        + [jax.ShapeDtypeStruct((2, slots, 3, local, share, width), bf16)]
        + [jax.ShapeDtypeStruct((count, 2, own_tokens, lanes), bf16)]
        + [jax.ShapeDtypeStruct(block, bf16)] * count,
        in_specs=[vmem] * 4 + [anywhere] * 3,
        out_specs=[vmem] * 3 + [anywhere] + [vmem] * (1 + count),
        scratch_shapes=[
            pltpu.VMEM((3, local, share, width), f32),
            pltpu.VMEM((count - 1, 3, local, share, width), bf16),
            pltpu.VMEM((rows, 128), f32),
            pltpu.VMEM((experts * capacity, 128), f32),
            pltpu.VMEM((count,) + block, bf16),
            pltpu.VMEM((tps, count) + block, bf16),
            pltpu.VMEM((local, tall, tps * columns), bf16),
            pltpu.VMEM((2, local, tall, width), f32),
            pltpu.VMEM((groups, local, tall, width), bf16),
            pltpu.VMEM((count, local, tall, columns), bf16),
            pltpu.VMEM((2, groups - 1, tall, 128), bf16),
            pltpu.VMEM((tps, local, tall, columns), bf16),
            sem((3,)), sem((count - 1,)), sem((2, items, 3, pieces)), sem((2, slots)),
            sem((count, 3, groups - 1)), sem((count, 3, pieces, groups - 1)),
            sem((count,)), sem((count,)), sem((1,)), sem((1,)),
            sem((count, pieces, groups)), sem((tps, pieces, groups)),
            sem((2, groups - 1)), sem((groups,)), sem((groups,)),
        ],
        compiler_params=pltpu.CompilerParams(
            collective_id=1, has_side_effects=True, vmem_limit_bytes=38 * 1024 * 1024
        ),
    )(
        tokens, routes.T, route_weights.T, norm_gain.reshape(rows // 128, 128),
        gate_weight, up_weight, down_weight,
    )
    arrived = [backs[0]] + [
        lax.ppermute(backs[d], "fs", list(enumerate(mates(count)[d])))
        for d in range(1, count)
    ]
    parts = max(1, shape[1] // 512)
    outs = pl.pallas_call(
        functools.partial(writer_kernel, parts),
        out_shape=[jax.ShapeDtypeStruct(shape, bf16)] * 3,
        in_specs=[vmem] * 3,
        out_specs=[anywhere] * 3,
        scratch_shapes=[sem((3, local, parts))],
        compiler_params=pltpu.CompilerParams(vmem_limit_bytes=1024 * 1024),
        cost_estimate=pl.CostEstimate(
            flops=10**11, bytes_accessed=12 * local * count * rows * width, transcendentals=0
        ),
    )(gate, up, down)
    mixed = pl.pallas_call(
        combine_kernel,
        out_shape=jax.ShapeDtypeStruct(tokens.shape, bf16),
        in_specs=[vmem] * (1 + count),
        out_specs=vmem,
        compiler_params=pltpu.CompilerParams(vmem_limit_bytes=8 * 1024 * 1024),
    )(weights, *arrived)
    return *outs, mixed


def on_device(tokens, routes, route_weights, norm_gain, gate_weight, up_weight, down_weight):
    groups, count, tps = (lax.axis_size(axis) for axis in ("grp", "fs", "tp"))
    experts, rows, width = gate_weight.shape
    own_tokens, columns = tokens.shape
    capacity = own_tokens * 5 // 16
    fits = (
        groups > 1 and 1 < count <= 8 and experts % count == 0 and rows == columns
        and count == tps and rows % (128 * groups) == 0 and width % 128 == 0
        and capacity % 8 == 0 and (experts // count * capacity) % 16 == 0
        and 6 * experts // count * count * rows * width <= 24 * 1024 * 1024
    )
    body = fused if fits else layered
    return tuple(
        body(tokens, routes, route_weights, norm_gain, gate_weight, up_weight, down_weight)
    )


def solution(mesh):
    in_specs = (
        P(("grp", "fs"), "tp"),
        P(("grp", "fs"), None),
        P(("grp", "fs"), None),
        P("fs"),
        P(None, "fs", "tp"),
        P(None, "fs", "tp"),
        P(None, "fs", "tp"),
    )
    out_specs = (
        P("fs", "grp", "tp"),
        P("fs", "grp", "tp"),
        P("fs", "grp", "tp"),
        P(("grp", "fs"), "tp"),
    )
    return jax.shard_map(
        on_device, mesh=mesh, in_specs=in_specs, out_specs=out_specs, check_vma=False
    )
```

```python
import functools

import jax
import jax.numpy as jnp
from jax import lax
from jax.experimental import pallas as pl
from jax.experimental.pallas import tpu as pltpu
from jax.sharding import PartitionSpec as P

epsilon = 1e-06
MESH = pl.DeviceIdType.MESH


def expert_slots(routes, experts, capacity):
    row_count = routes.shape[0] * routes.shape[1]
    flat_routes = routes.reshape(row_count)
    onehot = (flat_routes[:, None] == jnp.arange(experts, dtype=jnp.int32)[None, :]).astype(
        jnp.int32
    )
    earlier = jnp.cumsum(onehot, axis=0) - onehot
    position = jnp.sum(earlier * onehot, axis=1)
    return (flat_routes * capacity + position).reshape(routes.shape)


def dispatch(normed, slots, experts, capacity, copies, local_count):
    col_width = normed.shape[1]
    slot_ids = jnp.arange(experts * capacity, dtype=jnp.int32)
    select = jnp.any(slot_ids[:, None, None] == slots[None, :, :], axis=2).astype(jnp.bfloat16)
    packed = jnp.dot(select, normed, preferred_element_type=jnp.float32).astype(jnp.bfloat16)
    packed = jnp.broadcast_to(
        packed.reshape(experts, 1, capacity, col_width), (experts, copies, capacity, col_width)
    )
    return packed.reshape(experts * copies // local_count, local_count, capacity, col_width)


def combine(returned, slots, route_weights, experts, copies):
    capacity, col_width = (returned.shape[2], returned.shape[3])
    summed_up = jnp.sum(
        returned.reshape(experts, copies, capacity, col_width), axis=1, dtype=jnp.float32
    )
    selected = summed_up.reshape(experts * capacity, col_width)[slots]
    return jnp.sum(route_weights[:, :, None] * selected, axis=1)


def exchange_kernel(
    dims, gains, gate_w, up_w, down_w, gate_o, up_o, down_o,
    raw, stage, load_sem, send_sem, recv_sem, pass_send, pass_recv,
):
    groups, count, local, copies, rows, width, parts = dims
    weights, landing = (gate_w, up_w, down_w), (gate_o, up_o, down_o)
    y, z = lax.axis_index("grp"), lax.axis_index("fs")
    share = rows // groups
    piece = share // parts

    barrier = pltpu.get_barrier_semaphore()

    def greet(j, _):
        @pl.when(j != z)
        def _():
            pl.semaphore_signal(barrier, inc=1, device_id={"fs": j}, device_id_type=MESH)
        return 0

    lax.fori_loop(0, count, greet, 0)
    for other in range(1, groups):
        pl.semaphore_signal(
            barrier, inc=1, device_id={"grp": lax.rem(y + other, groups)}, device_id_type=MESH
        )

    def load(m, j, first, slot):
        if copies > 1:
            expert, column = j // copies, lax.rem(j, copies) * width
            column = pl.ds(pl.multiple_of(column, 128), width)
        else:
            expert, column = j * local, slice(None)
        return pltpu.make_async_copy(
            weights[m].at[pl.ds(expert, local), pl.ds(first, share), column],
            raw.at[slot], load_sem.at[slot],
        )

    def fold(m, slot, first, put):
        def one(i, _):
            l, q = i // parts, lax.rem(i, parts)
            at = pl.multiple_of(q * piece, piece)
            scaled = raw[slot, l, pl.ds(at, piece), :]
            if m < 2:
                scaled = scaled * gains[pl.ds(pl.multiple_of(first + at, piece), piece), :1]
            put(l, at, scaled.astype(jnp.bfloat16))
            return 0

        lax.fori_loop(0, local * parts, one, 0)

    def sending(j, m, i):
        l, q = i // parts, lax.rem(i, parts)
        at = pl.multiple_of(q * piece, piece)
        base = pl.multiple_of(z * rows + y * share + at, piece)
        return pltpu.make_async_remote_copy(
            src_ref=stage.at[j, m, l, pl.ds(at, piece), :],
            dst_ref=landing[m].at[l, pl.ds(base, piece), :],
            send_sem=send_sem.at[j, m, i],
            recv_sem=recv_sem.at[z, m, i],
            device_id={"fs": j}, device_id_type=MESH,
        )

    def passing(s, m, i, other):
        l, q = i // parts, lax.rem(i, parts)
        base = pl.multiple_of(s * rows + y * share + q * piece, piece)
        spot = landing[m].at[l, pl.ds(base, piece), :]
        return pltpu.make_async_remote_copy(
            src_ref=spot, dst_ref=spot,
            send_sem=pass_send.at[s, m, i, other - 1],
            recv_sem=pass_recv.at[s, m, i, other - 1],
            device_id={"grp": lax.rem(y + other, groups)}, device_id_type=MESH,
        )

    def arriving(s, m, i, other):
        l, q = i // parts, lax.rem(i, parts)
        giver = lax.rem(y + groups - other, groups)
        base = pl.multiple_of(s * rows + giver * share + q * piece, piece)
        spot = landing[m].at[l, pl.ds(base, piece), :]
        return pltpu.make_async_remote_copy(
            src_ref=spot, dst_ref=spot,
            send_sem=pass_send.at[s, m, i, other - 1],
            recv_sem=pass_recv.at[s, m, i, other - 1],
            device_id={"grp": giver}, device_id_type=MESH,
        )

    def landed(s, m, i):
        l, q = i // parts, lax.rem(i, parts)
        base = pl.multiple_of(s * rows + y * share + q * piece, piece)
        return pltpu.make_async_remote_copy(
            src_ref=landing[m].at[l, pl.ds(base, piece), :],
            dst_ref=landing[m].at[l, pl.ds(base, piece), :],
            send_sem=send_sem.at[s, m, i],
            recv_sem=recv_sem.at[s, m, i],
            device_id={"fs": s}, device_id_type=MESH,
        )

    mine = pl.multiple_of(y * share, share)
    pieces = local * parts

    def neighbours(body):
        def step(d, _):
            for j, there in ((z + d, z + d < count), (z - d, z - d >= 0)):
                @pl.when(there)
                def _():
                    body(j)
            return 0

        lax.fori_loop(1, count, step, 0)

    def send_phase(phase):
        def to(j):
            for m in phase:
                load(m, j, mine, m % 2).start()
            for m in phase:
                load(m, j, mine, m % 2).wait()

                def put(l, at, value):
                    stage[j, m, l, pl.ds(at, piece), :] = value

                fold(m, m % 2, mine, put)
            for m in phase:
                def go(i, _):
                    sending(j, m, i).start()
                    return 0

                lax.fori_loop(0, pieces, go, 0)

        neighbours(to)

    pl.semaphore_wait(barrier, count - 1 + groups - 1)
    send_phase((0, 1))
    send_phase((2,))

    for m in range(3):
        for g in range(groups):
            load(m, z, g * share, g % 2).start()
            load(m, z, g * share, g % 2).wait()

            def put(l, at, value):
                base = pl.multiple_of(z * rows + g * share + at, piece)
                landing[m][l, pl.ds(base, piece), :] = value

            fold(m, g % 2, g * share, put)

    def pass_phase(phase):
        def take(s):
            for m in phase:
                def one(i, _):
                    landed(s, m, i).wait_recv()
                    for other in range(1, groups):
                        passing(s, m, i, other).start()
                    return 0

                lax.fori_loop(0, pieces, one, 0)

        neighbours(take)

    pass_phase((0, 1))
    pass_phase((2,))

    def finish(s):
        for m in range(3):
            def one(i, _):
                for other in range(1, groups):
                    arriving(s, m, i, other).wait_recv()
                    passing(s, m, i, other).wait_send()
                sending(s, m, i).wait_send()
                return 0

            lax.fori_loop(0, pieces, one, 0)

    neighbours(finish)


def relay_kernel(
    dims, gains, gate_w, up_w, down_w, gate_o, up_o, down_o,
    raw, stage, transit, load_sem, send_sem, recv_sem, relay_sem, pass_send, pass_recv,
):
    groups, count, local, copies, rows, width, parts = dims
    weights, landing = (gate_w, up_w, down_w), (gate_o, up_o, down_o)
    y, z = lax.axis_index("grp"), lax.axis_index("fs")
    share = rows // groups
    piece = share // parts
    pieces = local * parts
    mine = pl.multiple_of(y * share, share)

    def real(way, place):
        return place if way == 0 else count - 1 - place

    barrier = pltpu.get_barrier_semaphore()
    for j, there in ((z + 1, z + 1 < count), (z - 1, z >= 1)):
        @pl.when(there)
        def _():
            pl.semaphore_signal(barrier, inc=1, device_id={"fs": j}, device_id_type=MESH)
    for other in range(1, groups):
        pl.semaphore_signal(
            barrier, inc=1, device_id={"grp": lax.rem(y + other, groups)}, device_id_type=MESH
        )

    def load(m, j, first, slot):
        if copies > 1:
            expert, column = j // copies, lax.rem(j, copies) * width
            column = pl.ds(pl.multiple_of(column, 128), width)
        else:
            expert, column = j * local, slice(None)
        return pltpu.make_async_copy(
            weights[m].at[pl.ds(expert, local), pl.ds(first, share), column],
            raw.at[slot], load_sem.at[slot],
        )

    def cut(i):
        return i // parts, pl.multiple_of(lax.rem(i, parts) * piece, piece)

    def fold(m, slot, first, put):
        def one(i, _):
            l, at = cut(i)
            scaled = raw[slot, l, pl.ds(at, piece), :]
            if m < 2:
                scaled = scaled * gains[pl.ds(pl.multiple_of(first + at, piece), piece), :1]
            put(l, at, scaled.astype(jnp.bfloat16))
            return 0

        lax.fori_loop(0, pieces, one, 0)

    def spot(m, l, at, source, giver):
        base = pl.multiple_of(source * rows + giver * share + at, piece)
        return landing[m].at[l, pl.ds(base, piece), :]

    def hop(way, src, sem, m, i, k, s, dd, final):
        l, at = cut(i)
        if final:
            dst = spot(m, l, at, real(way, s), y)
        else:
            slot = (k - s) * (count - 2 - k) + (count - 1 - dd)
            dst = transit.at[way, slot, m, l, pl.ds(at, piece), :]
        place = (k - s) * (count - 1 - k) + (count - 1 - dd)
        return pltpu.make_async_remote_copy(
            src_ref=src, dst_ref=dst, send_sem=sem,
            recv_sem=recv_sem.at[way, place, m, i],
            device_id={"fs": real(way, k + 1)}, device_id_type=MESH,
        )

    def start_hop(way, src, sem, m, i, k, s, dd):
        @pl.when(dd == k + 1)
        def _():
            hop(way, src, sem, m, i, k, s, dd, True).start()

        @pl.when(dd > k + 1)
        def _():
            hop(way, src, sem, m, i, k, s, dd, False).start()

    def passing(s, m, i, other):
        l, at = cut(i)
        ref = spot(m, l, at, s, y)
        return pltpu.make_async_remote_copy(
            src_ref=ref, dst_ref=ref,
            send_sem=pass_send.at[s, m, i, other - 1],
            recv_sem=pass_recv.at[s, m, i, other - 1],
            device_id={"grp": lax.rem(y + other, groups)}, device_id_type=MESH,
        )

    def arriving(s, m, i, other):
        l, at = cut(i)
        giver = lax.rem(y + groups - other, groups)
        ref = spot(m, l, at, s, giver)
        return pltpu.make_async_remote_copy(
            src_ref=ref, dst_ref=ref,
            send_sem=pass_send.at[s, m, i, other - 1],
            recv_sem=pass_recv.at[s, m, i, other - 1],
            device_id={"grp": giver}, device_id_type=MESH,
        )

    def send_phase(phase):
        def step(d, _):
            for way in (0, 1):
                k = real(way, z)
                dd = count - d
                j = real(way, dd)

                @pl.when(dd > k)
                def _():
                    for m in phase:
                        load(m, j, mine, m).start()
                    for m in phase:
                        load(m, j, mine, m).wait()

                        def put(l, at, value):
                            stage[j, m, l, pl.ds(at, piece), :] = value

                        fold(m, m, mine, put)

                        def go(i, _):
                            l, at = cut(i)
                            src = stage.at[j, m, l, pl.ds(at, piece), :]
                            start_hop(way, src, send_sem.at[j, m, i], m, i, k, k, dd)
                            return 0

                        lax.fori_loop(0, pieces, go, 0)
            return 0

        lax.fori_loop(1, count, step, 0)

    def own_block():
        for m in range(3):
            for g in range(groups):
                load(m, z, g * share, g % 2).start()
                load(m, z, g * share, g % 2).wait()

                def put(l, at, value):
                    stage[z, m, l, pl.ds(at, piece), :] = value

                fold(m, g % 2, g * share, put)
                base = pl.multiple_of(z * rows + g * share, share)
                keep = pltpu.make_async_copy(
                    stage.at[z, m], landing[m].at[:, pl.ds(base, share), :], load_sem.at[g % 2]
                )
                keep.start()
                keep.wait()

    def take_phase(phase):
        most = max(k * (count - k) for k in range(count))

        def take(item, _):
            for m in phase:
                def one(i, _):
                    l, at = cut(i)
                    for way in (0, 1):
                        take_piece(way, m, item, i, l, at)
                    return 0

                lax.fori_loop(0, pieces, one, 0)
            return 0

        lax.fori_loop(0, most, take, 0)

    def take_piece(way, m, item, i, l, at):
        k = real(way, z)

        @pl.when(item < k * (count - k))
        def _():
            s = k - 1 - item // (count - k)
            dd = count - 1 - lax.rem(item, count - k)
            source = real(way, s)

            def awaited(ref):
                pltpu.make_async_remote_copy(
                    src_ref=ref, dst_ref=ref, send_sem=send_sem.at[source, m, i],
                    recv_sem=recv_sem.at[way, item, m, i],
                    device_id={"fs": source}, device_id_type=MESH,
                ).wait_recv()

            @pl.when(dd == k)
            def _():
                awaited(spot(m, l, at, source, y))
                for other in range(1, groups):
                    passing(source, m, i, other).start()

            @pl.when(dd > k)
            def _():
                slot = (k - 1 - s) * (count - 1 - k) + (count - 1 - dd)
                ref = transit.at[way, slot, m, l, pl.ds(at, piece), :]
                awaited(ref)
                start_hop(way, ref, relay_sem.at[way, slot, m, i], m, i, k, s, dd)

    def sent(ref, sem):
        pltpu.make_async_remote_copy(
            src_ref=ref, dst_ref=ref, send_sem=sem, recv_sem=recv_sem.at[0, 0, 0, 0],
            device_id={"grp": lax.rem(y + 1, groups)}, device_id_type=MESH,
        ).wait_send()

    def finish():
        def block(t, _):
            s, i = t // pieces, lax.rem(t, pieces)
            l, at = cut(i)

            @pl.when(s != z)
            def _():
                for m in range(3):
                    for other in range(1, groups):
                        arriving(s, m, i, other).wait_recv()
                        passing(s, m, i, other).wait_send()
                    sent(stage.at[s, m, l, pl.ds(at, piece), :], send_sem.at[s, m, i])
            return 0

        lax.fori_loop(0, count * pieces, block, 0)

        def passed(t, _):
            slot, i = t // pieces, lax.rem(t, pieces)
            l, at = cut(i)
            for way in (0, 1):
                @pl.when(slot < z * (count - 1 - z))
                def _():
                    for m in range(3):
                        sent(
                            transit.at[way, slot, m, l, pl.ds(at, piece), :],
                            relay_sem.at[way, slot, m, i],
                        )
            return 0

        lax.fori_loop(0, transit.shape[1] * pieces, passed, 0)

    ends = (z == 0).astype(jnp.int32) + (z == count - 1).astype(jnp.int32)
    pl.semaphore_wait(barrier, 2 - ends + groups - 1)
    send_phase((0, 1, 2))
    own_block()
    take_phase((0, 1, 2))
    finish()


def exchange(norm_gain, gate_weight, up_weight, down_weight, groups, count, copies, local):
    experts, rows, columns = gate_weight.shape
    width = columns // copies
    share = rows // groups
    parts = max(1, share // 128)
    gains = jnp.broadcast_to(norm_gain[:, None], (rows, 128))
    shape = (local, count * rows, width)
    dims = (groups, count, local, copies, rows, width, parts)
    pieces = local * parts
    relaying = 1 < count <= 8 and groups > 1
    common = [
        pltpu.VMEM((3, local, share, width), jnp.float32),
        pltpu.VMEM((count, 3, local, share, width), jnp.bfloat16),
    ]
    sem = pltpu.SemaphoreType.DMA
    passes = [sem((count, 3, pieces, max(1, groups - 1)))] * 2
    if relaying:
        slots = max(1, max(k * (count - 1 - k) for k in range(count)))
        items = max(k * (count - k) for k in range(count))
        scratch = common + [
            pltpu.VMEM((2, slots, 3, local, share, width), jnp.bfloat16),
            sem((3,)), sem((count, 3, pieces)), sem((2, items, 3, pieces)),
            sem((2, slots, 3, pieces)),
        ] + passes
    else:
        scratch = common + [sem((2,))] + [sem((count, 3, pieces))] * 2 + passes
    return pl.pallas_call(
        functools.partial(relay_kernel if relaying else exchange_kernel, dims),
        out_shape=[jax.ShapeDtypeStruct(shape, jnp.bfloat16)] * 3,
        in_specs=[pl.BlockSpec(memory_space=pltpu.VMEM)]
        + [pl.BlockSpec(memory_space=pl.ANY)] * 3,
        out_specs=[pl.BlockSpec(memory_space=pl.ANY if relaying else pltpu.VMEM)] * 3,
        scratch_shapes=scratch,
        compiler_params=pltpu.CompilerParams(
            collective_id=0, has_side_effects=True, vmem_limit_bytes=60 * 1024 * 1024
        ),
    )(gains, gate_weight, up_weight, down_weight)


def layered(tokens, routes, route_weights, norm_gain, gate_weight, up_weight, down_weight):
    groups = lax.axis_size("grp")
    fs_count = lax.axis_size("fs")
    tp_count = lax.axis_size("tp")
    experts = gate_weight.shape[0]
    copies = max(1, fs_count // experts)
    local_count = max(1, experts // fs_count)
    capacity = tokens.shape[0] * 5 // 16

    gate_new, up_new, down_new = exchange(
        norm_gain, gate_weight, up_weight, down_weight, groups, fs_count, copies, local_count
    )
    slots = expert_slots(routes, experts, capacity)
    whole = lax.all_gather(tokens, "tp", axis=1, tiled=True)
    widened = whole.astype(jnp.float32)
    row_scale = lax.rsqrt(jnp.mean(widened * widened, axis=1, keepdims=True) + epsilon)
    normed = (widened * row_scale).astype(jnp.bfloat16)
    outgoing = dispatch(normed, slots, experts, capacity, copies, local_count)
    arrived = lax.all_to_all(outgoing, "fs", split_axis=0, concat_axis=0, tiled=True)
    gate_sums = jnp.einsum("slcd,ldf->slcf", arrived, gate_new, preferred_element_type=jnp.float32)
    up_sums = jnp.einsum("slcd,ldf->slcf", arrived, up_new, preferred_element_type=jnp.float32)
    hidden = (jax.nn.silu(gate_sums) * up_sums).astype(jnp.bfloat16)
    partial_value = jnp.einsum(
        "slcf,ldf->slcd", hidden, down_new, preferred_element_type=jnp.float32
    ).astype(jnp.bfloat16)
    by_columns = partial_value.reshape(
        partial_value.shape[:3] + (tp_count, partial_value.shape[3] // tp_count)
    )
    exchanged = lax.all_to_all(by_columns, "tp", split_axis=3, concat_axis=3, tiled=True)
    summed_up = jnp.sum(exchanged, axis=3, dtype=jnp.float32)
    handed = lax.all_to_all(
        summed_up.astype(jnp.bfloat16), "fs", split_axis=0, concat_axis=0, tiled=True
    ).astype(summed_up.dtype)
    combined = combine(handed, slots, route_weights, experts, copies)
    return (gate_new, up_new, down_new, combined.astype(jnp.bfloat16))


def far_first(count):
    table = []
    for z in range(count):
        right = [j for j in range(count - 1, z, -1)]
        left = [j for j in range(z)]
        ways, order = sorted((right, left), key=len, reverse=True), []
        for d in range(count):
            order += [way[d] for way in ways if d < len(way)]
        table.append(order)
    return table


def fused_kernel(
    dims, tokens, routes, route_weights, gains, gate_w, up_w, down_w,
    gate_o, up_o, down_o, mixed_o, transit,
    raw, stage, gain_col, scales, send_x, land_x, normed, sums, hidden, partial, across, summing, combine_w,
    send_ret, land_ret,
    load_sem, send_sem, recv_sem, relay_sem, pass_send, pass_recv,
    x_send, x_recv, xg_send, xg_recv, part_send, part_recv, ret_send, ret_recv,
    across_send, hid_send, hid_recv,
):
    groups, count, tps, local, rows, width, parts, experts, capacity = dims
    weights, landing = (gate_w, up_w, down_w), (gate_o, up_o, down_o)
    y, z, t = lax.axis_index("grp"), lax.axis_index("fs"), lax.axis_index("tp")
    share = rows // groups
    piece = share // parts
    pieces = local * parts
    mine = pl.multiple_of(y * share, share)
    table = far_first(count)
    block_rows = local * capacity
    own_tokens, columns = tokens.shape
    tall = count * capacity
    f32, bf16 = jnp.float32, jnp.bfloat16

    def ranked(r):
        return sum((z == k).astype(jnp.int32) * table[k][r] for k in range(count))

    def real(way, place):
        return place if way == 0 else count - 1 - place

    def remote(src, dst, send, recv, axis, index):
        return pltpu.make_async_remote_copy(
            src_ref=src, dst_ref=dst, send_sem=send, recv_sem=recv,
            device_id={axis: index}, device_id_type=MESH,
        )

    barrier = pltpu.get_barrier_semaphore()
    for axis, me, size in (("fs", z, count), ("grp", y, groups), ("tp", t, tps)):
        for other in range(1, size):
            pl.semaphore_signal(
                barrier, inc=1, device_id={axis: lax.rem(me + other, size)}, device_id_type=MESH
            )

    def load(m, j, first, slot):
        return pltpu.make_async_copy(
            weights[m].at[pl.ds(j * local, local), pl.ds(first, share), :],
            raw.at[slot], load_sem.at[slot],
        )

    def cut(i):
        return i // parts, pl.multiple_of(lax.rem(i, parts) * piece, piece)

    def fold(m, slot, first, put):
        def one(i, _):
            l, at = cut(i)
            scaled = raw[slot, l, pl.ds(at, piece), :]
            if m < 2:
                scaled = scaled * gain_col[pl.ds(pl.multiple_of(first + at, piece), piece), :1]
            put(l, at, scaled.astype(bf16))
            return 0

        lax.fori_loop(0, pieces, one, 0)

    def spot(m, l, at, source, giver):
        base = pl.multiple_of(source * rows + giver * share + at, piece)
        return landing[m].at[l, pl.ds(base, piece), :]

    def start_hop(way, src, sem, m, i, k, s, dd):
        l, at = cut(i)
        place = (k - s) * (count - 1 - k) + (count - 1 - dd)
        recv = recv_sem.at[way, place, m, i]

        @pl.when(dd == k + 1)
        def _():
            remote(src, spot(m, l, at, real(way, s), y), sem, recv, "fs", real(way, k + 1)).start()

        @pl.when(dd > k + 1)
        def _():
            slot = (k - s) * (count - 2 - k) + (count - 1 - dd)
            dst = transit.at[way, slot, m, l, pl.ds(at, piece), :]
            remote(src, dst, sem, recv, "fs", real(way, k + 1)).start()

    def passing(s, m, i, other):
        l, at = cut(i)
        ref = spot(m, l, at, s, y)
        return remote(
            ref, ref, pass_send.at[s, m, other - 1], pass_recv.at[s, m, i, other - 1],
            "grp", lax.rem(y + other, groups),
        )

    def arriving(s, m, i, other):
        l, at = cut(i)
        giver = lax.rem(y + groups - other, groups)
        ref = spot(m, l, at, s, giver)
        return remote(
            ref, ref, pass_send.at[s, m, other - 1], pass_recv.at[s, m, i, other - 1],
            "grp", giver,
        )

    def slot_rows():
        wanted = routes[...]
        expert_ids = lax.broadcasted_iota(jnp.int32, (experts, own_tokens), 0)
        onehots = [
            (expert_ids == wanted[k : k + 1, :]).astype(f32) for k in range(wanted.shape[0])
        ]
        before = lax.broadcasted_iota(jnp.int32, (own_tokens, own_tokens), 0)
        after = lax.broadcasted_iota(jnp.int32, (own_tokens, own_tokens), 1)
        upper = (before < after).astype(bf16)
        earlier = jnp.dot(sum(onehots).astype(bf16), upper, preferred_element_type=f32)
        found = []
        for k, onehot in enumerate(onehots):
            position = jnp.sum(earlier * onehot, axis=0, keepdims=True)
            earlier = earlier + onehot
            found.append(wanted[k : k + 1, :] * capacity + position.astype(jnp.int32))
        return found

    def pack():
        found = slot_rows()
        shape = (combine_w.shape[2], own_tokens)
        slot_ids = lax.broadcasted_iota(jnp.int32, shape, 0)
        chosen, weighed = jnp.zeros(shape, f32), jnp.zeros(shape, f32)
        for k, slot in enumerate(found):
            hit = slot_ids == slot
            chosen = jnp.where(hit, 1.0, chosen)
            weighed = weighed + jnp.where(hit, route_weights[k : k + 1, :], 0.0)
        packed = jnp.dot(chosen.astype(bf16), tokens[...], preferred_element_type=f32)
        packed = packed.astype(bf16)
        for j in range(count):
            send_x[j] = packed[j * block_rows : (j + 1) * block_rows, :]
        weighed = jnp.transpose(weighed)
        high = weighed.astype(bf16)
        combine_w[0] = high
        combine_w[1] = (weighed - high.astype(f32)).astype(bf16)

    def dispatching(j):
        return remote(send_x.at[j], land_x.at[t, z], x_send.at[j], x_recv.at[z], "fs", j)

    def dispatched(s):
        return remote(send_x.at[s], land_x.at[t, s], x_send.at[s], x_recv.at[s], "fs", s)

    def spreading(s, other):
        return remote(
            land_x.at[t, s], land_x.at[t, s], xg_send.at[0], xg_recv.at[0],
            "tp", lax.rem(t + other, tps),
        )

    def spread():
        ref = land_x.at[pl.ds(0, tps - 1)]
        return remote(ref, ref, xg_send.at[0], xg_recv.at[0], "tp", lax.rem(t + 1, tps))

    def elsewhere(body):
        for other in range(1, count):
            body(lax.rem(z + other, count))

    def normalise():
        for s in range(count):
            square = jnp.zeros((block_rows, 1), f32)
            for c in range(tps):
                part = land_x[c, s].astype(f32)
                square = square + jnp.sum(part * part, axis=1, keepdims=True)
            scales[s * block_rows : (s + 1) * block_rows, :] = jnp.broadcast_to(
                lax.rsqrt(square / (tps * columns) + epsilon), (block_rows, 128)
            )
        for c in range(tps):
            pile = [[] for _ in range(local)]
            for s in range(count):
                scale = scales[s * block_rows : (s + 1) * block_rows, :1]
                scaled = land_x[c, s].astype(f32) * scale
                for l in range(local):
                    pile[l].append(scaled[l * capacity : (l + 1) * capacity, :])
            for l in range(local):
                normed[l, :, c * columns : (c + 1) * columns] = jnp.concatenate(
                    pile[l], axis=0
                ).astype(bf16)

    tile = min(width, 256)

    def gate_up(s, first):
        def one(i, _):
            l, n = i // (width // tile), lax.rem(i, width // tile)
            base, at = pl.multiple_of(s * rows, rows), pl.multiple_of(n * tile, tile)
            x = normed[l, :, pl.ds(base, rows)]
            for m in range(2):
                w = landing[m][l, pl.ds(base, rows), pl.ds(at, tile)]
                value = jnp.dot(x, w, preferred_element_type=f32)
                if not first:
                    value = value + sums[m, l, :, pl.ds(at, tile)]
                sums[m, l, :, pl.ds(at, tile)] = value
            return 0

        lax.fori_loop(0, local * (width // tile), one, 0)

    def activate():
        def one(i, _):
            l, n = i // (width // tile), lax.rem(i, width // tile)
            at = pl.multiple_of(n * tile, tile)
            value = jax.nn.silu(sums[0, l, :, pl.ds(at, tile)]) * sums[1, l, :, pl.ds(at, tile)]
            hidden[y, l, :, pl.ds(at, tile)] = value.astype(bf16)
            return 0

        lax.fori_loop(0, local * (width // tile), one, 0)

    most = max(k * (count - k) for k in range(count))

    def comes_last(s):
        place = jnp.where(z > s, z, count - 1 - z)
        origin = jnp.where(z > s, s, count - 1 - s)
        arrival = (place - 1 - origin) * (count - place) + (count - 1 - place)
        return (z != s) & (arrival == most - 1)

    last = comes_last(t)

    def feature(giver, at):
        return pl.ds(pl.multiple_of(giver * share + at, piece), piece)

    def lending(other):
        return pltpu.make_async_remote_copy(
            src_ref=hidden.at[y, local - 1], dst_ref=hidden.at[y, local - 1],
            send_sem=hid_send.at[other], recv_sem=hid_recv.at[y], device_id={"grp": lax.rem(y + other, groups)},
            device_id_type=MESH,
        )

    def lent(other):
        giver = lax.rem(y + other, groups)
        ref = hidden.at[giver, local - 1]
        return remote(ref, ref, hid_send.at[other], hid_recv.at[giver], "grp", giver)

    def part_copy(s, i, giver):
        l, at = cut(i)
        col = feature(giver, at)
        return remote(
            partial.at[s, l, :, col], summing.at[t, l, :, col], part_send.at[s, i, giver],
            part_recv.at[t, i, giver], "tp", s,
        )

    final = pieces - 1

    def part_across(way, s, other):
        l, at = cut(final)
        return pltpu.make_async_remote_copy(
            src_ref=across.at[way, other - 1],
            dst_ref=summing.at[t, l, :, feature(y, at)],
            send_sem=across_send.at[way, other - 1], recv_sem=part_recv.at[t, final, y],
            device_id={"grp": lax.rem(y + other, groups), "tp": s}, device_id_type=MESH,
        )

    def part_here(peer, i, giver):
        l, at = cut(i)
        ref = summing.at[peer, l, :, feature(giver, at)]
        return remote(ref, ref, part_send.at[0, i, giver], part_recv.at[peer, i, giver], "tp", peer)

    def down_rows(group, s, i, giver):
        l, at = cut(i)
        base = pl.multiple_of(s * rows + giver * share + at, piece)
        return lax.dot_general(
            hidden[group, l], down_o[l, pl.ds(base, piece), :], (((1,), (1,)), ((), ())),
            preferred_element_type=f32,
        ).astype(bf16)

    def down_piece(s, i, givers):
        l, at = cut(i)
        for giver in givers:
            value = down_rows(y, s, i, giver)

            @pl.when(s == t)
            def _():
                summing[t, l, :, feature(giver, at)] = value

            @pl.when(s != t)
            def _():
                partial[s, l, :, feature(giver, at)] = value

        @pl.when(s != t)
        def _():
            for giver in givers:
                part_copy(s, i, giver).start()

    def down_last(way, s):
        for other in range(1, groups):
            across[way, other - 1] = down_rows(lax.rem(y + other, groups), s, final, y)
        down_piece(s, final, (y,))
        for other in range(1, groups):
            part_across(way, s, other).start()

    def close_piece(i):
        l, at = cut(i)
        for giver in range(groups):
            for other in range(1, tps):
                part_here(lax.rem(t + other, tps), i, giver).wait_recv()

            @pl.when((y != giver) & last & (i == final))
            def _():
                part_here(t, i, giver).wait_recv()

            col = feature(giver, at)
            value = summing[0, l, :, col].astype(f32)
            for peer in range(1, tps):
                value = value + summing[peer, l, :, col].astype(f32)
            sums[0, l, :, col] = value

    def returning(j):
        return remote(send_ret.at[j], land_ret.at[z], ret_send.at[j], ret_recv.at[z], "fs", j)

    def returned(s):
        return remote(send_ret.at[s], land_ret.at[s], ret_send.at[s], ret_recv.at[s], "fs", s)

    def give_back():
        for j in range(count):
            block = jnp.concatenate(
                [
                    sums[0, l, j * capacity : (j + 1) * capacity, :columns]
                    for l in range(local)
                ],
                axis=0,
            ).astype(bf16)

            @pl.when(z == j)
            def _():
                land_ret[j] = block

            @pl.when(z != j)
            def _():
                send_ret[j] = block
        for r in range(count - 1):
            returning(ranked(r)).start()

    sends = [(r, m, None) for r in range(count - 1) for m in (0, 1)]
    keeps = [(None, m, g) for m in (0, 1) for g in range(groups)]
    late = [(r, 2, None) for r in range(count - 1)] + [(None, 2, g) for g in range(groups)]
    units = sends + keeps + late
    slots = raw.shape[0]

    def unit_load(n):
        r, m, g = units[n]
        if g is None:
            return load(m, ranked(r), mine, n % slots)
        return load(m, z, g * share, n % slots)

    def send_unit(r, m):
        j = ranked(r)

        def go(i, _):
            l, at = cut(i)
            src = stage.at[r, m, l, pl.ds(at, piece), :]
            for way in (0, 1):
                @pl.when(j > z if way == 0 else j < z)
                def _():
                    start_hop(
                        way, src, send_sem.at[r], m, i, real(way, z), real(way, z),
                        real(way, j),
                    )
            return 0

        lax.fori_loop(0, pieces, go, 0)

    def do_unit(n):
        r, m, g = units[n]
        if n + slots - 1 < len(units):
            unit_load(n + slots - 1).start()
        unit_load(n).wait()
        if g is None:
            def put(l, at, value):
                stage[r, m, l, pl.ds(at, piece), :] = value

            fold(m, n % slots, mine, put)
        else:
            def put(l, at, value):
                base = pl.multiple_of(z * rows + g * share + at, piece)
                landing[m][l, pl.ds(base, piece), :] = value

            fold(m, n % slots, g * share, put)

    for n in range(slots - 1):
        unit_load(n).start()
    gain_rows = jnp.transpose(gains[...])
    for q in range(rows // 128):
        gain_col[q * 128 : (q + 1) * 128, :] = jnp.broadcast_to(gain_rows[:, q : q + 1], (128, 128))
    pack()
    pl.semaphore_wait(barrier, count - 1 + groups - 1 + tps - 1)
    elsewhere(lambda j: dispatching(j).start())
    for n in range(len(sends)):
        do_unit(n)
        send_unit(*units[n][:2])

    land_x[t, z] = send_x[z]
    for other in range(1, tps):
        spreading(z, other).start()

    def forward(s):
        dispatched(s).wait_recv()
        for other in range(1, tps):
            spreading(s, other).start()

    elsewhere(forward)
    for n in range(len(sends), len(units)):
        do_unit(n)
    spread().wait_recv()
    normalise()
    gate_up(z, True)

    def take_piece(way, m, item, i, ready, wide=None):
        k = real(way, z)
        l, at = cut(i)

        mine = True if wide is None else (2 * k >= count) == wide

        @pl.when((item < k * (count - k)) & mine)
        def _():
            s = k - 1 - item // (count - k)
            dd = count - 1 - lax.rem(item, count - k)
            source = real(way, s)

            def awaited(ref):
                remote(
                    ref, ref, send_sem.at[0], recv_sem.at[way, item, m, i], "fs", source
                ).wait_recv()

            @pl.when(dd == k)
            def _():
                awaited(spot(m, l, at, source, y))
                ready(source, m, i)

            @pl.when(dd > k)
            def _():
                slot = (k - 1 - s) * (count - 1 - k) + (count - 1 - dd)
                ref = transit.at[way, slot, m, l, pl.ds(at, piece), :]
                awaited(ref)
                start_hop(way, ref, relay_sem.at[way, slot], m, i, k, s, dd)

    def settled(way, item, body, wide=None):
        k = real(way, z)
        kept = jnp.maximum(item, 0)
        s = k - 1 - kept // (count - k)
        dd = count - 1 - lax.rem(kept, count - k)

        mine = True if wide is None else (2 * k >= count) == wide

        @pl.when((item >= 0) & (item < k * (count - k)) & (dd == k) & mine)
        def _():
            body(real(way, s))

    def pass_on(source, m, i):
        for other in range(1, groups):
            passing(source, m, i, other).start()

    def await_pass(s, m, i):
        for other in range(1, groups):
            arriving(s, m, i, other).wait_recv()

    def early_block(s):
        def one(i, _):
            for m in (0, 1):
                await_pass(s, m, i)
            return 0

        lax.fori_loop(0, pieces, one, 0)
        gate_up(s, False)

    def early(n, _):
        for m in (0, 1):
            def one(i, _):
                for way in (0, 1):
                    take_piece(way, m, n, i, pass_on)
                return 0

            lax.fori_loop(0, pieces, one, 0)
            if m == 0:
                for way in (0, 1):
                    settled(way, n - 1, early_block)

        @pl.when(n == min(1, most - 1))
        def _():
            for r in range(count - 1):
                send_unit(r, 2)
        return 0

    lax.fori_loop(0, most + 1, early, 0)
    activate()
    def at_middle(body):
        @pl.when((z * (count - z) == most) | ((count - 1 - z) * (z + 1) == most))
        def _():
            for other in range(1, groups):
                body(other)

    at_middle(lambda other: lending(other).start())

    def own_down(i, _):
        down_piece(z, i, range(groups))
        return 0

    lax.fori_loop(0, pieces, own_down, 0)

    def sent(ref, sem):
        remote(ref, ref, sem, recv_sem.at[0, 0, 0, 0], "grp", lax.rem(y + 1, groups)).wait_send()

    def drain():
        for r in range(count - 1):
            sent(stage.at[r], send_sem.at[r])
            for m in range(3):
                base = pl.multiple_of(ranked(r) * rows + y * share, share)
                for other in range(1, groups):
                    sent(
                        landing[m].at[:, pl.ds(base, share), :],
                        pass_send.at[ranked(r), m, other - 1],
                    )
        for slot in range(transit.shape[1]):
            @pl.when(slot < z * (count - 1 - z))
            def _():
                for way in (0, 1):
                    sent(transit.at[way, slot], relay_sem.at[way, slot])

    def own_close(i, _):
        close_piece(i)
        return 0

    def whole(p):
        return p // pieces, lax.rem(p, pieces)

    def work(s, i):
        await_pass(s, 2, i)
        down_piece(s, i, range(groups))

    def later(wide, span):
        def one(p, _):
            n, i = whole(p)

            @pl.when(p < span)
            def _():
                for way in (0, 1):
                    take_piece(way, 2, n, i, pass_on, wide)

            def trail(lag, body):
                n, i = whole(jnp.maximum(p - lag, 0))
                due = (p >= lag) & (p < span + lag)
                for way in (0, 1):
                    settled(way, jnp.where(due, n, -1), lambda s: body(s, i), wide)

            def close(s, i):
                @pl.when(s == t)
                def _():
                    close_piece(i)

            trail(1, work)
            trail(3, close)
            return 0

        lax.fori_loop(0, span + 3, one, 0)

    def ending(i, _):
        for way in (0, 1):
            take_piece(way, 2, most - 1, i, pass_on)
        for way in (0, 1):
            settled(way, jnp.where(i >= 1, most - 1, -1), lambda s: work(s, jnp.maximum(i - 1, 0)))
        return 0

    narrow = max([k * (count - k) for k in range(count) if 2 * k < count])
    later(False, narrow * pieces)
    at_middle(lambda other: lent(other).wait_recv())

    @pl.when(z == t)
    def _():
        lax.fori_loop(0, pieces, own_close, 0)

    later(True, (most - 1) * pieces)
    lax.fori_loop(0, final, ending, 0)
    for way in (0, 1):
        def use(source, m, i, way=way):
            down_last(way, source)
            pass_on(source, m, i)

        take_piece(way, 2, most - 1, final, use)
    for way in (0, 1):
        settled(way, most - 1, lambda s: work(s, final - 1))

    @pl.when(last)
    def _():
        lax.fori_loop(0, pieces, own_close, 0)

    give_back()
    drain()

    def drain_more(i, _):
        for s in range(count):
            for giver in range(groups):
                skipped = comes_last(s) & (y != giver) & (i == final)

                @pl.when((s != t) & jnp.logical_not(skipped))
                def _():
                    part_copy(s, i, giver).wait_send()
        for way in (0, 1):
            k = real(way, z)

            @pl.when((k * (count - k) == most) & (i == final))
            def _():
                await_pass(real(way, 0), 2, i)
                for other in range(1, groups):
                    part_across(way, real(way, 0), other).wait_send()
        return 0

    lax.fori_loop(0, pieces, drain_more, 0)
    at_middle(lambda other: lending(other).wait_send())
    elsewhere(lambda j: dispatching(j).wait_send())
    spread().wait_send()

    elsewhere(lambda s: returned(s).wait_recv())
    back = land_ret[...].reshape(experts * capacity, columns)
    used = experts * capacity
    value = jnp.dot(combine_w[0, :, :used], back, preferred_element_type=f32)
    value = value + jnp.dot(combine_w[1, :, :used], back, preferred_element_type=f32)
    mixed_o[...] = value.astype(bf16)
    elsewhere(lambda j: returning(j).wait_send())


def writer_kernel(parts, *refs):
    ins, outs, sem = refs[:4], refs[4:8], refs[8]
    local, high = ins[0].shape[:2]
    step = high // parts

    def copy(k, l, i):
        at = pl.ds(i * step, step)
        return pltpu.make_async_copy(ins[k].at[l, at, :], outs[k].at[l, at, :], sem.at[k, l, i])

    small = pltpu.make_async_copy(ins[3], outs[3], sem.at[3, 0, 0])
    jobs = [copy(k, l, i) for k in range(3) for l in range(local) for i in range(parts)] + [small]
    for job in jobs:
        job.start()
    for job in jobs:
        job.wait()


def fused(tokens, routes, route_weights, norm_gain, gate_weight, up_weight, down_weight):
    groups, count, tps = (lax.axis_size(axis) for axis in ("grp", "fs", "tp"))
    experts, rows, width = gate_weight.shape
    local, own_tokens, columns = experts // count, *tokens.shape
    capacity = own_tokens * 5 // 16
    share = rows // groups
    parts = share // 128
    pieces = local * parts
    tall = count * capacity
    dims = (groups, count, tps, local, rows, width, parts, experts, capacity)
    shape = (local, count * rows, width)
    slots = max(1, max(k * (count - 1 - k) for k in range(count)))
    items = max(k * (count - k) for k in range(count))
    bf16, f32, sem = jnp.bfloat16, jnp.float32, pltpu.SemaphoreType.DMA
    vmem, anywhere = pl.BlockSpec(memory_space=pltpu.VMEM), pl.BlockSpec(memory_space=pl.ANY)
    block = (local * capacity, columns)
    gate, up, down, mixed, _ = pl.pallas_call(
        functools.partial(fused_kernel, dims),
        out_shape=[pltpu.VMEM(shape, bf16)] * 3
        + [pltpu.VMEM(tokens.shape, bf16)]
        + [jax.ShapeDtypeStruct((2, slots, 3, local, share, width), bf16)],
        in_specs=[vmem] * 4 + [anywhere] * 3,
        out_specs=[vmem] * 4 + [anywhere],
        scratch_shapes=[
            pltpu.VMEM((3, local, share, width), f32),
            pltpu.VMEM((count - 1, 3, local, share, width), bf16),
            pltpu.VMEM((rows, 128), f32),
            pltpu.VMEM((experts * capacity, 128), f32),
            pltpu.VMEM((count,) + block, bf16),
            pltpu.VMEM((tps, count) + block, bf16),
            pltpu.VMEM((local, tall, tps * columns), bf16),
            pltpu.VMEM((2, local, tall, width), f32),
            pltpu.VMEM((groups, local, tall, width), bf16),
            pltpu.VMEM((count, local, tall, columns), bf16),
            pltpu.VMEM((2, groups - 1, tall, 128), bf16),
            pltpu.VMEM((tps, local, tall, columns), bf16),
            pltpu.VMEM((2, own_tokens, -(-experts * capacity // 128) * 128), bf16),
            pltpu.VMEM((count,) + block, bf16),
            pltpu.VMEM((count,) + block, bf16),
            sem((3,)), sem((count - 1,)), sem((2, items, 3, pieces)), sem((2, slots)),
            sem((count, 3, groups - 1)), sem((count, 3, pieces, groups - 1)),
            sem((count,)), sem((count,)), sem((1,)), sem((1,)),
            sem((count, pieces, groups)), sem((tps, pieces, groups)), sem((count,)), sem((count,)),
            sem((2, groups - 1)), sem((groups,)), sem((groups,)),
        ],
        compiler_params=pltpu.CompilerParams(
            collective_id=1, has_side_effects=True, vmem_limit_bytes=38 * 1024 * 1024
        ),
    )(
        tokens, routes.T, route_weights.T, norm_gain.reshape(rows // 128, 128),
        gate_weight, up_weight, down_weight,
    )
    parts = max(1, shape[1] // 512)
    return pl.pallas_call(
        functools.partial(writer_kernel, parts),
        out_shape=[jax.ShapeDtypeStruct(shape, bf16)] * 3
        + [jax.ShapeDtypeStruct(tokens.shape, bf16)],
        in_specs=[vmem] * 4,
        out_specs=[anywhere] * 4,
        scratch_shapes=[sem((4, local, parts))],
        compiler_params=pltpu.CompilerParams(vmem_limit_bytes=1024 * 1024),
    )(gate, up, down, mixed)


def on_device(tokens, routes, route_weights, norm_gain, gate_weight, up_weight, down_weight):
    groups, count, tps = (lax.axis_size(axis) for axis in ("grp", "fs", "tp"))
    experts, rows, width = gate_weight.shape
    own_tokens, columns = tokens.shape
    capacity = own_tokens * 5 // 16
    fits = (
        groups > 1 and 1 < count <= 8 and experts % count == 0 and rows == columns
        and count == tps and rows % (128 * groups) == 0 and width % 128 == 0
        and capacity % 8 == 0 and (experts // count * capacity) % 16 == 0
        and 6 * experts // count * count * rows * width <= 24 * 1024 * 1024
    )
    body = fused if fits else layered
    return tuple(
        body(tokens, routes, route_weights, norm_gain, gate_weight, up_weight, down_weight)
    )


def solution(mesh):
    in_specs = (
        P(("grp", "fs"), "tp"),
        P(("grp", "fs"), None),
        P(("grp", "fs"), None),
        P("fs"),
        P(None, "fs", "tp"),
        P(None, "fs", "tp"),
        P(None, "fs", "tp"),
    )
    out_specs = (
        P("fs", "grp", "tp"),
        P("fs", "grp", "tp"),
        P("fs", "grp", "tp"),
        P(("grp", "fs"), "tp"),
    )
    return jax.shard_map(
        on_device, mesh=mesh, in_specs=in_specs, out_specs=out_specs, check_vma=False
    )
```
